32 devices in a mesh: sp: 8 (over z, y), tp: 4 (over x, core).
Axes of the slice: x: 2, y: 2, z: 4, core: 2. Of those that a mesh axis runs over, the one named last changes fastest.
Arguments:
- proj_value: bfloat16 [4096, 2016], P('sp', 'tp'), may hold values from -6 to 6
- proj_gate: bfloat16 [4096, 2016], P('sp', 'tp'), may hold values from -8 to 8
- conv_saved: bfloat16 [4096, 2016], P('sp', 'tp'), may hold values from -12 to 12
- conv_taps: bfloat16 [31, 2016], P(None, 'tp'), may hold values from -1 to 1
- norm_gain: bfloat16 [2016], P('tp'), may hold values from 0.099609375 to 1.8984375
- out_weight: bfloat16 [2016, 2016], P('tp'), may hold values from -0.125 to 0.125
- cotangent: bfloat16 [4096, 2016], P('sp'), may hold values from -6 to 6
Outputs:
- grad_value: bfloat16 [4096, 2016], P('sp', 'tp')
- grad_gate: bfloat16 [4096, 2016], P('sp', 'tp')
- grad_out_weight: float32 [2016, 2016], P('tp', 'sp')
- grad_taps: float32 [31, 2016], P(None, 'tp')
The draws below stay inside these ranges and needn't reach their ends.
All inputs are finite; a program needn't handle non-finite values.
Results may differ from the reference program's by a relative error of at most 0.003.
Values sent between devices are 32-bit elements; how exact they have to be, the bound alone decides.
A program may use at most 64 MiB of HBM per device.

```python
import math
import jax
import jax.numpy as jnp
from jax import lax

D = 2016
KERNEL = 31
TOKENS = 4096


def draw_conv_saved(key, part):
    key_phase, key_rough, key_base = jax.random.split(jax.random.fold_in(key, 7), 3)
    channel = jnp.arange(D, dtype=jnp.float32) / D
    phase = jax.random.uniform(key_phase, (), jnp.float32, 0.0, 2.0 * math.pi)
    smooth = jnp.exp(1.2 * jnp.sin(2.0 * math.pi * 1.5 * channel + phase))
    rough = jnp.exp(jax.random.uniform(key_rough, (D,), jnp.float32, -0.4, 0.4))
    values = jax.random.normal(key_base, (TOKENS, D), jnp.float32) * smooth * rough
    return jnp.clip(values, -12.0, 12.0).astype(jnp.bfloat16)


def spiked(entries, stream_key, source, target, blocks, factor):
    owner, partner = [(jnp.arange(entries.shape[position]) // (entries.shape[position] // blocks)).reshape([-1 if axis == position else 1 for axis in range(entries.ndim)]) for position in (source, target)]
    chosen = jax.random.permutation(stream_key, blocks)[partner]
    strong = (owner == chosen) | (owner == (partner + blocks // 2) % blocks)
    return jnp.where(strong, factor * entries, entries)


def steps_of(key, extent, cuts, least, top_value):
    def one(position, parts):
        draws = jax.random.uniform(jax.random.fold_in(jax.random.fold_in(key, 6), position), (parts,), jnp.float32, least / len(cuts), top_value / len(cuts))
        return jnp.repeat(jnp.exp(draws), extent[position] // parts).reshape((-1,) + (1,) * (len(extent) - position - 1))

    loudness = one(*cuts[0])
    for cut in cuts[1:]:
        loudness = loudness * one(*cut)
    return loudness


def bell_draw(own_key, shape, deviation, bound, cuts=(), kind=jnp.bfloat16):
    drawn = jax.random.normal(own_key, shape, jnp.float32) * deviation
    if len(cuts) > 0:
        drawn = steps_of(own_key, shape, cuts, -0.22, 0.18) * drawn
    return jnp.clip(drawn, min=-bound, max=bound).astype(kind)


def heavy_noise(own_key, shape, width, limit, cuts, heavy, held_as=jnp.bfloat16):
    values = width * jax.random.normal(own_key, shape, jnp.float32)
    if cuts:
        values = values * steps_of(own_key, shape, cuts, -0.22, 0.18)
    return jnp.clip(spiked(values, jax.random.fold_in(own_key, 3), *heavy), -limit, limit).astype(held_as)


def setup_inputs(seed: int = 0) -> dict:
    arg_keys = jax.random.split(jax.random.key(seed), 8)
    return {
        "proj_value": bell_draw(arg_keys[0], (TOKENS, D), 1.0, 6.0, ((0, 8), (1, 4))),
        "proj_gate": bell_draw(arg_keys[1], (TOKENS, D), 1.5, 8.0, ((0, 8), (1, 4))),
        "conv_saved": draw_conv_saved(jax.random.fold_in(arg_keys[7], 71), 0),
        "conv_taps": bell_draw(arg_keys[3], (KERNEL, D), KERNEL ** -0.5, 1.0, ((1, 4),)),
        "norm_gain": jnp.clip(1.0 + 0.18 * jax.random.normal(arg_keys[4], (D,), jnp.float32), 0.099609375, 1.8984375).astype(jnp.bfloat16),
        "out_weight": bell_draw(arg_keys[5], (D, D), D ** -0.5, 0.125, ((0, 4),)),
        "cotangent": heavy_noise(arg_keys[6], (TOKENS, D), 1.0, 6.0, ((0, 8),), (0, 1, 8, 2.0)),
    }


norm_eps = 1e-05

def reference(proj_value, proj_gate, conv_saved, conv_taps, norm_gain, out_weight, cotangent):
    conv_f = conv_saved.astype(jnp.float32)
    row_mean = lax.optimization_barrier(jnp.sum(conv_f, axis=1)) / D
    row_var = lax.optimization_barrier(jnp.sum(conv_f * conv_f, axis=1)) / D - row_mean * row_mean
    inv_std = lax.rsqrt(row_var + norm_eps)
    centered = (conv_f - row_mean[:, None]) * inv_std[:, None]
    gain_f = norm_gain.astype(jnp.float32)
    normed = centered * gain_f
    gate_norm = jax.nn.sigmoid(normed)
    activated = (normed * gate_norm).astype(jnp.bfloat16)
    grad_scale = 1.0 / math.sqrt(TOKENS)
    grad_out_weight = jnp.dot(activated.T, cotangent, preferred_element_type=jnp.float32) * grad_scale
    d_act = jnp.dot(cotangent, out_weight.T, preferred_element_type=jnp.float32)
    d_hat = d_act * gate_norm * (1.0 + normed * (1.0 - gate_norm)) * gain_f
    first = lax.optimization_barrier(jnp.sum(d_hat, axis=1)) / D
    second = lax.optimization_barrier(jnp.sum(d_hat * centered, axis=1)) / D
    d_conv = inv_std[:, None] * (d_hat - first[:, None] - centered * second[:, None])
    overhang = KERNEL - 1
    extended = jnp.concatenate([d_conv, jnp.zeros((overhang, D), jnp.float32)], axis=0)
    gate_proj = jax.nn.sigmoid(proj_gate.astype(jnp.float32))
    gated = proj_value.astype(jnp.float32) * gate_proj
    taps_f = conv_taps.astype(jnp.float32)
    d_glu = jnp.zeros((TOKENS, D), jnp.float32)
    tap_rows = []
    for offset in range(KERNEL):
        shifted = extended[overhang - offset:overhang - offset + TOKENS]
        d_glu = d_glu + taps_f[offset] * shifted
        tap_rows.append(lax.optimization_barrier(jnp.sum(gated * shifted, axis=0)))
    grad_taps = jnp.stack(tap_rows) * grad_scale
    grad_value = (d_glu * gate_proj).astype(jnp.bfloat16)
    grad_gate = (d_glu * gated * (1.0 - gate_proj)).astype(jnp.bfloat16)
    return (grad_value, grad_gate, grad_out_weight, grad_taps)
```

```python
import functools
import math

import jax
import jax.numpy as jnp
from jax import lax
from jax.experimental import pallas as pl
from jax.experimental.pallas import tpu as pltpu
from jax.sharding import PartitionSpec as P

norm_eps = 1e-05
MESH = pl.DeviceIdType.MESH
f32 = jnp.float32
pieces = 4


def line_order(length):
    rows = []
    for place in range(length):
        side = 1 if 2 * place >= length else -1
        rows.append(sorted(range(length), key=lambda d: (-abs(d - place), -side * (d - place))))
    return rows


def split_rows(ch):
    chunk = max((ch * 33 + 640) // 1280, 1) * 8
    return chunk * pieces, ch - chunk * pieces


def lookup(table, place):
    value = table[0]
    for i in range(1, len(table)):
        value = jnp.where(place == i, table[i], value)
    return value


def finish(v_in, g_in, w_in, t_in, v_out, g_out, w_out, t_out, ss):
    pairs = [(v_in, v_out), (g_in, g_out), (w_in, w_out), (t_in, t_out)]
    copies = [pltpu.make_async_copy(a, b, ss.at[i]) for i, (a, b) in enumerate(pairs)]
    for c in copies:
        c.start()
    for c in copies:
        c.wait()


def kernel(
    n_sp, n_tp, fold, pv_h, pg_h, conv, taps, gain, weight_h, cot_h,
    out_v, out_g, out_w, out_t,
    pv, pg, weight, cot, in_sems, gain_c, gated_s, d_glu_s, act_t, d_act, ext, shifted, cols, cols2, term, got_y, got_r, got_l, low_r, low_l, low_y,
    stat, stat_in, mom, mom_in, grad_acc, g_own, g_mid, g_up, g_dn, g_up_out, g_dn_out, g_yin, taps_b,
    stat_ss, stat_rs, mom_ss, mom_rs, y_ss, y_rs, r_ss, r_rs, l_ss, l_rs,
    lr_ss, lr_rs, ll_ss, ll_rs, ly_ss, ly_rs,
    halo_ss, halo_rs, gu_ss, gu_rs, gd_ss, gd_rs, gy_ss, gy_rs,
):
    s = lax.axis_index("sp")
    t = lax.axis_index("tp")
    n_z = n_sp // fold
    z = s // fold
    y = s % fold
    other_y = 1 - y
    width, rows = cot.shape
    ch = conv.shape[0]
    part = out_w.shape[1]
    n_taps = taps.shape[0]
    scale = 1.0 / math.sqrt(rows * n_sp)
    blk = 128
    n_blk = rows // blk
    top, low = split_rows(ch)
    end = jnp.logical_or(z == 0, z == n_z - 1)
    mid = jnp.logical_and(z > 0, z < n_z - 1)

    loads = [
        pltpu.make_async_copy(a, b, in_sems.at[i])
        for i, (a, b) in enumerate([(cot_h, cot), (weight_h, weight), (pv_h, pv), (pg_h, pg)])
    ]
    for c in loads:
        c.start()

    barrier = pltpu.get_barrier_semaphore()

    def greet(s_to, t_to):
        pl.semaphore_signal(barrier, inc=1, device_id=(s_to, t_to), device_id_type=MESH)

    for i in range(1, n_tp):
        greet(s, lax.rem(t + i, n_tp))
    greet(z * fold + other_y, t)

    @pl.when(z > 0)
    def _():
        greet(s - fold, t)

        @pl.when(y == 0)
        def _():
            greet(s - 1, t)

    @pl.when(z < n_z - 1)
    def _():
        greet(s + fold, t)

        @pl.when(y == fold - 1)
        def _():
            greet(s + 1, t)

    def put_sums(ref, i, first, second):
        ref[pl.ds(i, 1), :] = jnp.sum(first, axis=0, keepdims=True)
        ref[pl.ds(n_blk + i, 1), :] = jnp.sum(second, axis=0, keepdims=True)

    if stat.shape[0] > 2 * n_blk:
        stat[...] = jnp.zeros_like(stat)
        mom[...] = jnp.zeros_like(mom)

    @pl.loop(0, n_blk)
    def _(i):
        at = pl.ds(pl.multiple_of(i * blk, blk), blk)
        c = conv[:, at].astype(f32)
        put_sums(stat, i, c, c * c)

    below = jnp.where(z > 0, jnp.where(y == 0, 2, 1), 0)
    above = jnp.where(z < n_z - 1, jnp.where(y == fold - 1, 2, 1), 0)
    pl.semaphore_wait(barrier, n_tp + below + above)

    def tp_copies(src, dst, ss, rs):
        return [
            pltpu.make_async_remote_copy(
                src_ref=src, dst_ref=dst.at[i - 1], send_sem=ss.at[i - 1], recv_sem=rs.at[i - 1],
                device_id=(s, lax.rem(t + i, n_tp)), device_id_type=MESH,
            )
            for i in range(1, n_tp)
        ]

    stat_copies = tp_copies(stat, stat_in, stat_ss, stat_rs)
    for c in stat_copies:
        c.start()

    gain_c[...] = jnp.broadcast_to(gain[...].astype(f32).reshape(1, ch), (128, ch)).T
    loads[0].wait()
    loads[1].wait()
    wide_blk = 256 if rows % 256 == 0 else 128

    @pl.loop(0, rows // wide_blk)
    def _(i):
        at = pl.ds(pl.multiple_of(i * wide_blk, wide_blk), wide_blk)
        d_act[:, at] = jnp.dot(weight[...], cot[:, at], preferred_element_type=f32)

    for c in stat_copies:
        c.wait()
    total = stat[...]
    for i in range(n_tp - 1):
        total = total + stat_in[i]
    mean = total[:n_blk] / width
    inv = lax.rsqrt(total[n_blk:2 * n_blk] / width - mean * mean + norm_eps)
    for i in range(n_blk):
        cols[0:1, i * blk:(i + 1) * blk] = mean[i:i + 1]
        cols[1:2, i * blk:(i + 1) * blk] = inv[i:i + 1]

    @pl.loop(0, n_blk)
    def _(i):
        at = pl.ds(pl.multiple_of(i * blk, blk), blk)
        c = conv[:, at].astype(f32)
        normed = (c - cols[0:1, at]) * cols[1:2, at] * gain_c[...]
        act_t[:, at] = (normed * jax.nn.sigmoid(normed)).astype(jnp.bfloat16)

    orders = line_order(n_z)
    dest = [lookup([orders[i][k] for i in range(n_z)], z) for k in range(n_z)]

    chunk = top // pieces

    def piece(h):
        return pl.ds(h * chunk, chunk)

    def y_copy(k, h):
        sem = dest[k] * pieces + h
        return pltpu.make_async_remote_copy(
            src_ref=term.at[dest[k] * fold + other_y, piece(h), :], dst_ref=got_y.at[dest[k], piece(h), :],
            send_sem=y_ss.at[sem], recv_sem=y_rs.at[sem],
            device_id=(z * fold + other_y, t), device_id_type=MESH,
        )

    y_copies = [[y_copy(k, h) for h in range(pieces)] for k in range(n_z)]

    def y_start(k, first=0, last=pieces):
        for h in range(first, last):
            y_copies[k][h].start()

    def make_term(j):
        term[j] = lax.dot_general(
            act_t[...], cot[j * part:(j + 1) * part, :], (((1,), (1,)), ((), ())),
            preferred_element_type=f32,
        )

    lead = dest[0] * fold + other_y
    second = dest[0] * fold + y
    leads = sorted({orders[i][0] * fold + o for i in range(n_z) for o in range(fold)})

    def make_one_of(place):
        for j in leads:
            @pl.when(place == j)
            def _():
                make_term(j)

    def line_copy(d, h, up):
        buf, ss, rs = (got_r, r_ss, r_rs) if up else (got_l, l_ss, l_rs)
        to = z + 1 if up else z - 1
        to = jnp.clip(to, 0, n_z - 1)
        return pltpu.make_async_remote_copy(
            src_ref=term.at[d * fold + y, piece(h), :], dst_ref=buf.at[d, piece(h), :],
            send_sem=ss.at[d * pieces + h], recv_sem=rs.at[d * pieces + h],
            device_id=(to * fold + y, t), device_id_type=MESH,
        )

    def add_into(d, h, buf):
        own = d * fold + y
        term[own, piece(h), :] = term[own, piece(h), :] + buf[d, piece(h), :]

    def hop(k, h):
        d = dest[k]
        y_copies[k][h].wait_recv()
        add_into(d, h, got_y)

        @pl.when(d > z)
        def _():
            @pl.when(z > 0)
            def _():
                line_copy(d, h, True).wait_recv()
                add_into(d, h, got_r)

            line_copy(d, h, True).start()

        @pl.when(d < z)
        def _():
            @pl.when(z < n_z - 1)
            def _():
                line_copy(d, h, False).wait_recv()
                add_into(d, h, got_l)

            line_copy(d, h, False).start()

    def low_copy(d, up):
        buf, ss, rs = (low_r, lr_ss, lr_rs) if up else (low_l, ll_ss, ll_rs)
        to = jnp.clip(z + 1 if up else z - 1, 0, n_z - 1)
        return pltpu.make_async_remote_copy(
            src_ref=term.at[pl.ds(d * fold, fold), pl.ds(top, low), :], dst_ref=buf.at[d],
            send_sem=ss.at[d], recv_sem=rs.at[d], device_id=(to * fold + y, t), device_id_type=MESH,
        )

    def low_take(d, up):
        low_copy(d, up).wait_recv()
        buf = low_r if up else low_l
        at = pl.ds(d * fold, fold)
        term[at, pl.ds(top, low), :] = term[at, pl.ds(top, low), :] + buf[d]

    def low_hop(k):
        d = dest[k]

        @pl.when(d > z)
        def _():
            @pl.when(z > 0)
            def _():
                low_take(d, True)

            low_copy(d, True).start()

        @pl.when(d < z)
        def _():
            @pl.when(z < n_z - 1)
            def _():
                low_take(d, False)

            low_copy(d, False).start()

    low_swap = pltpu.make_async_remote_copy(
        src_ref=term.at[z * fold + other_y, pl.ds(top, low), :], dst_ref=low_y,
        send_sem=ly_ss, recv_sem=ly_rs, device_id=(z * fold + other_y, t), device_id_type=MESH,
    )

    def low_end():
        @pl.when(z > 0)
        def _():
            low_take(z, True)

        @pl.when(z < n_z - 1)
        def _():
            low_take(z, False)

        low_swap.start()

    make_one_of(lead)
    y_start(0)
    make_one_of(second)

    @pl.when(end)
    def _():
        low_hop(0)

    for j in range(n_sp):
        if j in leads:
            @pl.when(jnp.logical_and(lead != j, second != j))
            def _():
                make_term(j)
        else:
            make_term(j)

    @pl.when(end)
    def _():
        for k in range(1, n_z - 1):
            low_hop(k)

    @pl.loop(0, n_blk)
    def _(i):
        at = pl.ds(pl.multiple_of(i * blk, blk), blk)
        c = conv[:, at].astype(f32)
        centered = (c - cols[0:1, at]) * cols[1:2, at]
        normed = centered * gain_c[...]
        gate = jax.nn.sigmoid(normed)
        d_hat = d_act[:, at] * gate * (1.0 + normed * (1.0 - gate)) * gain_c[...]
        d_act[:, at] = d_hat
        put_sums(mom, i, d_hat, d_hat * centered)

    mom_copies = tp_copies(mom, mom_in, mom_ss, mom_rs)
    for c in mom_copies:
        c.start()
    for k in range(n_taps):
        taps_b[k] = jnp.broadcast_to(taps[k:k + 1, :].astype(f32), (8, ch))
    grad_acc[...] = jnp.zeros_like(grad_acc)
    loads[2].wait()
    loads[3].wait()

    @pl.loop(0, n_blk)
    def _(i):
        at = pl.ds(pl.multiple_of(i * blk, blk), blk)
        gated_s[at, :] = (pv[:, at].astype(f32) * jax.nn.sigmoid(pg[:, at].astype(f32))).T

    for c in mom_copies:
        c.wait()
    total = mom[...]
    for i in range(n_tp - 1):
        total = total + mom_in[i]
    total = total / width
    for i in range(n_blk):
        cols2[0:1, i * blk:(i + 1) * blk] = total[i:i + 1]
        cols2[1:2, i * blk:(i + 1) * blk] = total[n_blk + i:n_blk + i + 1]

    @pl.loop(0, n_blk)
    def _(i):
        at = pl.ds(pl.multiple_of(i * blk, blk), blk)
        c = conv[:, at].astype(f32)
        inv_std = cols[1:2, at]
        centered = (c - cols[0:1, at]) * inv_std
        ext[at, :] = (inv_std * (d_act[:, at] - cols2[0:1, at] - centered * cols2[1:2, at])).T

    reach = 32
    back = jnp.maximum(s - 1, 0)
    halo = pltpu.make_async_remote_copy(
        src_ref=ext.at[pl.ds(0, reach), :], dst_ref=ext.at[pl.ds(rows, reach), :],
        send_sem=halo_ss, recv_sem=halo_rs, device_id=(back, t), device_id_type=MESH,
    )

    @pl.when(s > 0)
    def _():
        halo.start()

    y_start(1)

    def shift_block(i):
        start = pl.multiple_of(i * reach, reach)
        win = ext[pl.ds(start, reach + 8), :]
        for o in range(8):
            shifted[o, pl.ds(start, reach), :] = win[o:o + reach]

    lanes = [(lo, min(128, ch - lo)) for lo in range(0, ch, 128)]

    def conv_blocks(first, last):
        for lo, wide in lanes:
            ln = slice(lo, lo + wide)

            def body(i, accs):
                start = pl.multiple_of(i * reach, reach)
                at = pl.ds(start, reach)
                gated = gated_s[at, ln]
                d_glu = jnp.zeros((reach, wide), f32)
                out = []
                for o in range(n_taps):
                    x = shifted[o % 8, pl.ds(pl.multiple_of(start + 8 * (o // 8), 8), reach), ln]
                    tap = taps_b[n_taps - 1 - o, :, ln]
                    d_glu = d_glu + jnp.concatenate([tap] * (reach // 8), axis=0) * x
                    prod = gated * x
                    acc = accs[o]
                    for q in range(reach // 8):
                        acc = acc + prod[8 * q:8 * q + 8]
                    out.append(acc)
                d_glu_s[at, ln] = d_glu
                return tuple(out)

            accs = tuple(grad_acc[n_taps - 1 - o, :, ln] for o in range(n_taps))
            accs = lax.fori_loop(first, last, body, accs)
            for o in range(n_taps):
                grad_acc[n_taps - 1 - o, :, ln] = accs[o]

    n_row = rows // reach

    @pl.loop(0, n_row - 1)
    def _(i):
        shift_block(i)

    half = (n_row - 2) // 2
    conv_blocks(0, half)

    @pl.when(end)
    def _():
        hop(0, 0)
        hop(0, 1)

    @pl.when(mid)
    def _():
        low_hop(0)

    conv_blocks(half, n_row - 2)

    @pl.when(s < n_sp - 1)
    def _():
        halo.wait_recv()

    @pl.when(s == n_sp - 1)
    def _():
        ext[pl.ds(rows, reach), :] = jnp.zeros((reach, ch), f32)

    shift_block(n_row - 1)
    win = ext[pl.ds(rows, reach), :]
    for o in range(8):
        shifted[o, pl.ds(rows, reach - 8), :] = win[o:o + reach - 8]
    conv_blocks(n_row - 2, n_row)

    for k in range(n_taps):
        g_own[k:k + 1, :] = jnp.sum(grad_acc[k], axis=0, keepdims=True)
    for k in range(n_taps, g_own.shape[0]):
        g_own[k:k + 1, :] = jnp.zeros((1, ch), f32)

    def taps_copy(src, up):
        dst, ss, rs = (g_up, gu_ss, gu_rs) if up else (g_dn, gd_ss, gd_rs)
        to = jnp.clip(z + 1 if up else z - 1, 0, n_z - 1)
        return pltpu.make_async_remote_copy(
            src_ref=src, dst_ref=dst, send_sem=ss, recv_sem=rs,
            device_id=(to * fold + y, t), device_id_type=MESH,
        )

    def taps_pass(up):
        src = g_up if up else g_dn
        out = g_up_out if up else g_dn_out
        taps_copy(g_own, up).wait_recv()
        out[...] = g_own[...] + src[...]
        taps_copy(out, up).start()

    @pl.when(z == 0)
    def _():
        g_up[...] = jnp.zeros_like(g_up)
        taps_copy(g_own, True).start()

    @pl.when(z == n_z - 1)
    def _():
        g_dn[...] = jnp.zeros_like(g_dn)
        taps_copy(g_own, False).start()

    y_start(2, 0, pieces if n_z > 3 else 2)

    @pl.loop(0, n_blk)
    def _(i):
        at = pl.ds(pl.multiple_of(i * blk, blk), blk)
        gate = jax.nn.sigmoid(pg[:, at].astype(f32))
        d_glu = d_glu_s[at, :].T
        out_v[:, at] = (d_glu * gate).astype(jnp.bfloat16)
        out_g[:, at] = (d_glu * (pv[:, at].astype(f32) * gate) * (1.0 - gate)).astype(jnp.bfloat16)

    @pl.when(end)
    def _():
        hop(0, 2)
        hop(0, 3)
        for k in range(1, n_z - 2):
            for h in range(pieces):
                hop(k, h)

    @pl.when(mid)
    def _():
        for k in range(n_z - 2, 0, -1):
            low_hop(k)
        hop(0, 0)
        hop(0, 1)

        @pl.when(2 * z < n_z)
        def _():
            taps_pass(True)

        @pl.when(2 * z >= n_z)
        def _():
            taps_pass(False)

        hop(0, 2)
        hop(0, 3)

    low_end()
    if n_z > 3:
        y_start(n_z - 1, 0, 2)

    @pl.when(end)
    def _():
        for h in range(pieces):
            hop(n_z - 2, h)

    @pl.when(mid)
    def _():
        @pl.when(2 * z < n_z)
        def _():
            taps_pass(False)

        @pl.when(2 * z >= n_z)
        def _():
            taps_pass(True)

        for h in range(pieces):
            hop(1, h)

    @pl.when(z == 0)
    def _():
        taps_copy(g_own, False).wait_recv()

    @pl.when(z == n_z - 1)
    def _():
        taps_copy(g_own, True).wait_recv()

    g_mid[...] = g_own[...] + g_up[...] + g_dn[...]
    gy = pltpu.make_async_remote_copy(
        src_ref=g_mid, dst_ref=g_yin, send_sem=gy_ss, recv_sem=gy_rs,
        device_id=(z * fold + other_y, t), device_id_type=MESH,
    )
    gy.start()
    y_start(n_z - 1, 2, pieces)

    @pl.when(mid)
    def _():
        for k in range(2, n_z - 1):
            for h in range(pieces):
                hop(k, h)

    own = z * fold + y
    low_swap.wait()
    out_w[top:, :] = (term[own, top:, :] + low_y[...]) * scale
    for h in range(pieces):
        y_copies[n_z - 1][h].wait_recv()
        add_into(z, h, got_y)

        @pl.when(z > 0)
        def _():
            line_copy(z, h, True).wait_recv()
            add_into(z, h, got_r)

        @pl.when(z < n_z - 1)
        def _():
            line_copy(z, h, False).wait_recv()
            add_into(z, h, got_l)

        out_w[piece(h), :] = term[own, piece(h), :] * scale

    gy.wait()
    out_t[...] = ((g_mid[...] + g_yin[...]) * scale)[:n_taps]
    for k in range(n_z):
        for h in range(pieces):
            y_copies[k][h].wait_send()

    @pl.when(z < n_z - 1)
    def _():
        taps_copy(g_own, True).wait_send()

    @pl.when(z > 0)
    def _():
        taps_copy(g_own, False).wait_send()

    @pl.when(s > 0)
    def _():
        halo.wait_send()

    for k in range(n_z - 1):
        d = dest[k]

        @pl.when(d > z)
        def _():
            for h in range(pieces):
                line_copy(d, h, True).wait_send()
            low_copy(d, True).wait_send()

        @pl.when(d < z)
        def _():
            for h in range(pieces):
                line_copy(d, h, False).wait_send()
            low_copy(d, False).wait_send()


def fused(n_sp, n_tp, proj_value, proj_gate, conv_saved, conv_taps, norm_gain, out_weight, cotangent):
    fold = 2
    n_z = n_sp // fold
    rows, width = cotangent.shape
    ch = conv_saved.shape[1]
    n_taps = conv_taps.shape[0]
    part = width // n_sp
    top, low = split_rows(ch)
    sums = -(-2 * (rows // 128) // 8) * 8
    dma = pltpu.SemaphoreType.DMA
    V = pltpu.VMEM
    bf = jnp.bfloat16
    vm = pl.BlockSpec(memory_space=pltpu.VMEM)
    hb = pl.BlockSpec(memory_space=pl.ANY)
    grad_value, grad_gate, grad_weight, grad_taps = pl.pallas_call(
        functools.partial(kernel, n_sp, n_tp, fold),
        out_shape=(V((ch, rows), bf), V((ch, rows), bf), V((ch, part), f32), V((n_taps, ch), f32)),
        in_specs=[hb, hb, vm, vm, vm, hb, hb],
        out_specs=[vm] * 4,
        scratch_shapes=[
            V((ch, rows), bf), V((ch, rows), bf), V((ch, width), bf), V((width, rows), bf), dma((4,)),
            V((ch, 128), f32), V((rows, ch), f32), V((rows, ch), f32),
            V((ch, rows), bf), V((ch, rows), f32), V((rows + 32, ch), f32), V((8, rows + 32, ch), f32),
            V((8, rows), f32), V((8, rows), f32),
            V((n_sp, ch, part), f32), V((n_z, top, part), f32), V((n_z, top, part), f32),
            V((n_z, top, part), f32),
            V((n_z, fold, low, part), f32), V((n_z, fold, low, part), f32), V((low, part), f32),
            V((sums, 128), f32), V((n_tp - 1, sums, 128), f32),
            V((sums, 128), f32), V((n_tp - 1, sums, 128), f32),
            V((n_taps, 8, ch), f32), *[V((32, ch), f32)] * 7, V((n_taps, 8, ch), f32),
            dma((n_tp - 1,)), dma((n_tp - 1,)), dma((n_tp - 1,)), dma((n_tp - 1,)),
            *[dma((pieces * n_z,))] * 6,
            dma((n_z,)), dma((n_z,)), dma((n_z,)), dma((n_z,)), dma, dma,
            *[dma] * 8,
        ],
        compiler_params=pltpu.CompilerParams(
            collective_id=0, has_side_effects=True, vmem_limit_bytes=56 * 1024 * 1024
        ),
    )(
        proj_value.T, proj_gate.T, conv_saved.T, conv_taps, norm_gain, out_weight,
        cotangent.T,
    )
    results = (grad_value, grad_gate, grad_weight, grad_taps)
    grad_value, grad_gate, grad_weight, grad_taps = pl.pallas_call(
        finish,
        out_shape=tuple(jax.ShapeDtypeStruct(r.shape, r.dtype) for r in results),
        in_specs=[vm] * 4,
        out_specs=[hb] * 4,
        scratch_shapes=[dma((4,))],
    )(*[pltpu.with_memory_space_constraint(r, pltpu.VMEM) for r in results])
    return grad_value.T, grad_gate.T, grad_weight, grad_taps


def passed_along(block, axis, distance):
    devices = range(lax.axis_size(axis))
    route = [(i - distance, i) for i in devices if i - distance in devices]
    return lax.ppermute(block, axis, route)


def local(proj_value, proj_gate, conv_saved, conv_taps, norm_gain, out_weight, cotangent):
    model_width = cotangent.shape[1]
    tok_rows = cotangent.shape[0]
    tap_count = conv_taps.shape[0]
    overhang = tap_count - 1
    grad_scale = 1.0 / math.sqrt(tok_rows * lax.axis_size("sp"))
    conv_f = conv_saved.astype(jnp.float32)
    totals = lax.psum((jnp.sum(conv_f, axis=1), jnp.sum(conv_f * conv_f, axis=1)), "tp")
    row_mean = totals[0] / model_width
    row_var = totals[1] / model_width - row_mean * row_mean
    inv_std = lax.rsqrt(row_var + norm_eps)
    centered = (conv_f - row_mean[:, None]) * inv_std[:, None]
    gain_f = norm_gain.astype(jnp.float32)
    normed = centered * gain_f
    gate_norm = jax.nn.sigmoid(normed)
    activated = (normed * gate_norm).astype(jnp.bfloat16)
    contract_rows = (((0,), (0,)), ((), ()))
    whole_term = lax.dot_general(
        cotangent, activated, contract_rows, preferred_element_type=jnp.float32
    )
    shard_grad = lax.psum_scatter(whole_term, "sp", scatter_dimension=0, tiled=True)
    grad_out_weight = shard_grad.T * grad_scale
    d_act = lax.dot_general(
        cotangent, out_weight, (((1,), (1,)), ((), ())), preferred_element_type=jnp.float32
    )
    d_hat = d_act * gate_norm * (1.0 + normed * (1.0 - gate_norm)) * gain_f
    moments = lax.psum((jnp.sum(d_hat, axis=1), jnp.sum(d_hat * centered, axis=1)), "tp")
    first = moments[0] / model_width
    second = moments[1] / model_width
    d_conv = inv_std[:, None] * (d_hat - first[:, None] - centered * second[:, None])
    ahead = passed_along(d_conv[:overhang], "sp", -1)
    extended = jnp.concatenate([d_conv, ahead], axis=0)
    gate_proj = jax.nn.sigmoid(proj_gate.astype(jnp.float32))
    gated = proj_value.astype(jnp.float32) * gate_proj
    taps_f = conv_taps.astype(jnp.float32)
    d_glu = jnp.zeros_like(d_conv)
    tap_rows = []
    for offset in range(tap_count):
        shifted = extended[overhang - offset : overhang - offset + tok_rows]
        d_glu = d_glu + taps_f[offset] * shifted
        tap_rows.append(jnp.sum(gated * shifted, axis=0))
    grad_taps = lax.psum(jnp.stack(tap_rows), "sp") * grad_scale
    grad_value = (d_glu * gate_proj).astype(jnp.bfloat16)
    grad_gate = (d_glu * gated * (1.0 - gate_proj)).astype(jnp.bfloat16)
    return (grad_value, grad_gate, grad_out_weight, grad_taps)


def solution(mesh):
    in_specs = (
        P("sp", "tp"),
        P("sp", "tp"),
        P("sp", "tp"),
        P(None, "tp"),
        P("tp"),
        P("tp", None),
        P("sp", None),
    )
    out_specs = (P("sp", "tp"), P("sp", "tp"), P("tp", "sp"), P(None, "tp"))
    n_sp, n_tp = mesh.shape["sp"], mesh.shape["tp"]

    def step(*args):
        rows, width = args[6].shape
        ch, n_taps = args[2].shape[1], args[3].shape[0]
        small = n_sp % 2 == 0 and 6 <= n_sp <= 8 and width % n_sp == 0 and n_tp > 1
        if small and rows % 128 == 0 and rows >= 128 and ch % 8 == 0 and ch >= 64 and 24 < n_taps <= 31:
            return fused(n_sp, n_tp, *args)
        return local(*args)

    return jax.shard_map(step, mesh=mesh, in_specs=in_specs, out_specs=out_specs, check_vma=False)
```

```python
import functools
import math

import jax
import jax.numpy as jnp
from jax import lax
from jax.experimental import pallas as pl
from jax.experimental.pallas import tpu as pltpu
from jax.sharding import PartitionSpec as P

norm_eps = 1e-05
MESH = pl.DeviceIdType.MESH
f32 = jnp.float32
pieces = 4


def line_order(length):
    rows = []
    for place in range(length):
        side = 1 if 2 * place >= length else -1
        rows.append(sorted(range(length), key=lambda d: (-abs(d - place), -side * (d - place))))
    return rows


def split_rows(ch):
    units = ch * 17 // 20 // 8
    sizes = [8 * (units // pieces + (i < units % pieces)) for i in range(pieces)]
    return sizes, sum(sizes), ch - sum(sizes)


def lookup(table, place):
    value = table[0]
    for i in range(1, len(table)):
        value = jnp.where(place == i, table[i], value)
    return value


def finish(v_in, g_in, w_in, t_in, v_out, g_out, w_out, t_out, ss):
    pairs = [(v_in, v_out), (g_in, g_out), (w_in, w_out), (t_in, t_out)]
    copies = [pltpu.make_async_copy(a, b, ss.at[i]) for i, (a, b) in enumerate(pairs)]
    for c in copies:
        c.start()
    for c in copies:
        c.wait()


def kernel(
    n_sp, n_tp, fold, pv_h, pg_h, conv_h, taps_h, gain_h, weight_h, cot_h,
    out_v, out_g, out_w, out_t,
    conv, taps, gain, pv, pg, weight, cot, in_sems, gain_c, gated_s, d_glu_s, act_t, d_act, ext, shifted, cols, cols2, term, got_y, got_line, low_in, low_y,
    stat, stat_in, mom, mom_in, grad_acc, g_own, g_mid, g_up, g_dn, g_up_out, g_dn_out, g_yin, taps_b, edge_out, edge_in, edge_sums, edge_sums_in,
    stat_ss, stat_rs, mom_ss, mom_rs, y_ss, y_rs, line_ss, line_rs,
    low_ss, low_rs, ly_ss, ly_rs, edge_ss, edge_rs,
    gu_ss, gu_rs, gd_ss, gd_rs, gy_ss, gy_rs,
):
    s = lax.axis_index("sp")
    t = lax.axis_index("tp")
    n_z = n_sp // fold
    z = s // fold
    y = s % fold
    other_y = 1 - y
    width, rows = cot.shape
    ch = conv.shape[0]
    part = out_w.shape[1]
    n_taps = taps.shape[0]
    scale = 1.0 / math.sqrt(rows * n_sp)
    blk = 128
    n_blk = rows // blk
    sizes, top, low = split_rows(ch)
    end = jnp.logical_or(z == 0, z == n_z - 1)
    mid = jnp.logical_and(z > 0, z < n_z - 1)

    loads = [
        pltpu.make_async_copy(a, b, in_sems.at[i])
        for i, (a, b) in enumerate([
            (cot_h, cot), (weight_h, weight), (pv_h, pv), (pg_h, pg), (conv_h, conv), (gain_h, gain), (taps_h, taps)
        ])
    ]
    loads[4].start()

    barrier = pltpu.get_barrier_semaphore()

    def greet(s_to, t_to):
        pl.semaphore_signal(barrier, inc=1, device_id=(s_to, t_to), device_id_type=MESH)

    for i in range(1, n_tp):
        greet(s, lax.rem(t + i, n_tp))
    greet(z * fold + other_y, t)

    @pl.when(z > 0)
    def _():
        greet(s - fold, t)

        @pl.when(y == 0)
        def _():
            greet(s - 1, t)

    @pl.when(z < n_z - 1)
    def _():
        greet(s + fold, t)

        @pl.when(y == fold - 1)
        def _():
            greet(s + 1, t)

    for i in (0, 1, 5, 2, 3, 6):
        loads[i].start()

    def put_sums(ref, i, first, second):
        ref[pl.ds(i, 1), :] = jnp.sum(first, axis=0, keepdims=True)
        ref[pl.ds(n_blk + i, 1), :] = jnp.sum(second, axis=0, keepdims=True)

    if stat.shape[0] > 2 * n_blk:
        stat[...] = jnp.zeros_like(stat)
        mom[...] = jnp.zeros_like(mom)

    loads[4].wait()

    @pl.loop(0, n_blk)
    def _(i):
        at = pl.ds(pl.multiple_of(i * blk, blk), blk)
        c = conv[:, at].astype(f32)
        put_sums(stat, i, c, c * c)

    below = jnp.where(z > 0, jnp.where(y == 0, 2, 1), 0)
    above = jnp.where(z < n_z - 1, jnp.where(y == fold - 1, 2, 1), 0)
    pl.semaphore_wait(barrier, n_tp + below + above)

    def tp_copies(src, dst, ss, rs):
        return [
            pltpu.make_async_remote_copy(
                src_ref=src, dst_ref=dst.at[i - 1], send_sem=ss, recv_sem=rs,
                device_id=(s, lax.rem(t + i, n_tp)), device_id_type=MESH,
            )
            for i in range(1, n_tp)
        ]

    def tp_wait(dst, ss, rs):
        pltpu.make_async_remote_copy(
            src_ref=dst, dst_ref=dst, send_sem=ss, recv_sem=rs,
            device_id=(s, lax.rem(t + 1, n_tp)), device_id_type=MESH,
        ).wait()

    for c in tp_copies(stat, stat_in, stat_ss, stat_rs):
        c.start()

    reach = 32
    back = jnp.maximum(s - 1, 0)

    def edge_copy(i):
        src, dst = (edge_sums, edge_sums_in) if i == 2 else (edge_out.at[i], edge_in.at[i])
        return pltpu.make_async_remote_copy(
            src_ref=src, dst_ref=dst, send_sem=edge_ss.at[i], recv_sem=edge_rs.at[i],
            device_id=(back, t), device_id_type=MESH,
        )

    def edge_send(i):
        @pl.when(s > 0)
        def _():
            edge_copy(i).start()

    edge_out[0] = conv[:, :blk].astype(f32).T[:reach]
    edge_send(0)
    loads[5].wait()
    gain_c[...] = jnp.broadcast_to(gain[...].astype(f32).reshape(1, ch), (128, ch)).T
    loads[0].wait()
    loads[1].wait()
    wide_blk = 256 if rows % 256 == 0 else 128

    d_act[:, :wide_blk] = jnp.dot(weight[...], cot[:, :wide_blk], preferred_element_type=f32)
    edge_out[1] = d_act[:, :blk].T[:reach]
    edge_send(1)

    @pl.loop(1, rows // wide_blk)
    def _(i):
        at = pl.ds(pl.multiple_of(i * wide_blk, wide_blk), wide_blk)
        d_act[:, at] = jnp.dot(weight[...], cot[:, at], preferred_element_type=f32)

    tp_wait(stat_in, stat_ss, stat_rs)
    total = stat[...]
    for i in range(n_tp - 1):
        total = total + stat_in[i]
    mean = total[:n_blk] / width
    inv = lax.rsqrt(total[n_blk:2 * n_blk] / width - mean * mean + norm_eps)
    for i in range(n_blk):
        cols[0:1, i * blk:(i + 1) * blk] = mean[i:i + 1]
        cols[1:2, i * blk:(i + 1) * blk] = inv[i:i + 1]

    orders = line_order(n_z)
    dest = [lookup([orders[i][k] for i in range(n_z)], z) for k in range(n_z)]

    firsts = [sum(sizes[:h]) for h in range(pieces)]

    def piece(h):
        return pl.ds(firsts[h], sizes[h])

    def y_copy(k, h):
        sem = dest[k] * pieces + h
        return pltpu.make_async_remote_copy(
            src_ref=term.at[dest[k] * fold + other_y, piece(h), :], dst_ref=got_y.at[dest[k], piece(h), :],
            send_sem=y_ss, recv_sem=y_rs.at[sem],
            device_id=(z * fold + other_y, t), device_id_type=MESH,
        )

    y_copies = [[y_copy(k, h) for h in range(pieces)] for k in range(n_z)]

    def y_start(k, first=0, last=pieces):
        for h in range(first, last):
            y_copies[k][h].start()

    def make_term(j, at=slice(None)):
        term[j, at, :] = lax.dot_general(
            act_t[at, :], cot[j * part:(j + 1) * part, :], (((1,), (1,)), ((), ())),
            preferred_element_type=f32,
        )

    lead = dest[0] * fold + other_y
    second = dest[0] * fold + y
    leads = sorted({orders[i][0] * fold + o for i in range(n_z) for o in range(fold)})

    def make_one_of(place, at=slice(None)):
        for j in leads:
            @pl.when(place == j)
            def _():
                make_term(j, at)

    def line_copy(d, h, up):
        slot = d + 1 if up else d
        to = z + 1 if up else z - 1
        to = jnp.clip(to, 0, n_z - 1)
        return pltpu.make_async_remote_copy(
            src_ref=term.at[d * fold + y, piece(h), :], dst_ref=got_line.at[slot, piece(h), :],
            send_sem=line_ss, recv_sem=line_rs.at[slot * pieces + h],
            device_id=(to * fold + y, t), device_id_type=MESH,
        )

    def add_into(d, h, buf, slot):
        own = d * fold + y
        term[own, piece(h), :] = term[own, piece(h), :] + buf[slot, piece(h), :]

    def line_take(d, h, up):
        line_copy(d, h, up).wait_recv()
        add_into(d, h, got_line, d + 1 if up else d)

    def hop(k, h):
        d = dest[k]
        y_copies[k][h].wait_recv()
        add_into(d, h, got_y, d)

        @pl.when(d > z)
        def _():
            @pl.when(z > 0)
            def _():
                line_take(d, h, True)

            line_copy(d, h, True).start()

        @pl.when(d < z)
        def _():
            @pl.when(z < n_z - 1)
            def _():
                line_take(d, h, False)

            line_copy(d, h, False).start()

    def low_copy(d, up):
        slot = d + 1 if up else d
        to = jnp.clip(z + 1 if up else z - 1, 0, n_z - 1)
        return pltpu.make_async_remote_copy(
            src_ref=term.at[pl.ds(d * fold, fold), pl.ds(top, low), :], dst_ref=low_in.at[slot],
            send_sem=low_ss, recv_sem=low_rs.at[slot], device_id=(to * fold + y, t), device_id_type=MESH,
        )

    def low_take(d, up):
        low_copy(d, up).wait_recv()
        at = pl.ds(d * fold, fold)
        term[at, pl.ds(top, low), :] = term[at, pl.ds(top, low), :] + low_in[d + 1 if up else d]

    def low_hop(k):
        d = dest[k]

        @pl.when(d > z)
        def _():
            @pl.when(z > 0)
            def _():
                low_take(d, True)

            low_copy(d, True).start()

        @pl.when(d < z)
        def _():
            @pl.when(z < n_z - 1)
            def _():
                low_take(d, False)

            low_copy(d, False).start()

    low_swap = pltpu.make_async_remote_copy(
        src_ref=term.at[z * fold + other_y, pl.ds(top, low), :], dst_ref=low_y,
        send_sem=ly_ss, recv_sem=ly_rs, device_id=(z * fold + other_y, t), device_id_type=MESH,
    )

    def low_end():
        @pl.when(z > 0)
        def _():
            low_take(z, True)

        @pl.when(z < n_z - 1)
        def _():
            low_take(z, False)

        low_swap.start()

    def activate(at):
        c = conv[at, :].astype(f32)
        gains = jnp.concatenate([gain_c[at, :]] * n_blk, axis=1)
        normed = (c - cols[0:1, :]) * cols[1:2, :] * gains
        act_t[at, :] = (normed * jax.nn.sigmoid(normed)).astype(jnp.bfloat16)

    def lead_piece(h):
        at = slice(firsts[h], firsts[h] + sizes[h])
        activate(at)
        make_one_of(lead, at)
        y_copies[0][h].start()

    lead_piece(0)
    activate(slice(top, None))
    make_one_of(lead, slice(top, None))
    make_one_of(second, slice(top, None))

    @pl.when(end)
    def _():
        low_hop(0)

    for h in range(1, pieces):
        lead_piece(h)
    make_one_of(second, slice(0, top))

    for j in range(n_sp):
        if j in leads:
            @pl.when(jnp.logical_and(lead != j, second != j))
            def _():
                make_term(j)
        else:
            make_term(j)

    @pl.when(end)
    def _():
        for k in range(1, n_z - 1):
            low_hop(k)

    @pl.loop(0, n_blk)
    def _(i):
        at = pl.ds(pl.multiple_of(i * blk, blk), blk)
        c = conv[:, at].astype(f32)
        centered = (c - cols[0:1, at]) * cols[1:2, at]
        normed = centered * gain_c[...]
        gate = jax.nn.sigmoid(normed)
        d_hat = d_act[:, at] * gate * (1.0 + normed * (1.0 - gate)) * gain_c[...]
        d_act[:, at] = d_hat
        put_sums(mom, i, d_hat, d_hat * centered)

    for c in tp_copies(mom, mom_in, mom_ss, mom_rs):
        c.start()
    loads[6].wait()
    for k in range(n_taps):
        taps_b[k] = jnp.broadcast_to(taps[k:k + 1, :].astype(f32), (8, ch))
    grad_acc[...] = jnp.zeros_like(grad_acc)
    loads[2].wait()
    loads[3].wait()

    @pl.loop(0, n_blk)
    def _(i):
        at = pl.ds(pl.multiple_of(i * blk, blk), blk)
        gated_s[at, :] = (pv[:, at].astype(f32) * jax.nn.sigmoid(pg[:, at].astype(f32))).T

    tp_wait(mom_in, mom_ss, mom_rs)
    total = mom[...]
    for i in range(n_tp - 1):
        total = total + mom_in[i]
    total = total / width
    for i in range(n_blk):
        cols2[0:1, i * blk:(i + 1) * blk] = total[i:i + 1]
        cols2[1:2, i * blk:(i + 1) * blk] = total[n_blk + i:n_blk + i + 1]

    edge_sums[...] = jnp.zeros_like(edge_sums)
    edge_sums[0:2, :] = cols[0:2, :blk]
    edge_sums[2:4, :] = cols2[0:2, :blk]
    edge_send(2)
    y_start(1)

    @pl.loop(0, n_blk)
    def _(i):
        at = pl.ds(pl.multiple_of(i * blk, blk), blk)
        c = conv[:, at].astype(f32)
        inv_std = cols[1:2, at]
        centered = (c - cols[0:1, at]) * inv_std
        ext[at, :] = (inv_std * (d_act[:, at] - cols2[0:1, at] - centered * cols2[1:2, at])).T

    def shift_block(i):
        start = pl.multiple_of(i * reach, reach)
        win = ext[pl.ds(start, reach + 8), :]
        for o in range(8):
            shifted[o, pl.ds(start, reach), :] = win[o:o + reach]

    lanes = [(lo, min(128, ch - lo)) for lo in range(0, ch, 128)]

    def conv_blocks(first, last):
        for lo, wide in lanes:
            ln = slice(lo, lo + wide)

            def body(i, accs):
                start = pl.multiple_of(i * reach, reach)
                at = pl.ds(start, reach)
                gated = gated_s[at, ln]
                d_glu = jnp.zeros((reach, wide), f32)
                out = []
                for o in range(n_taps):
                    x = shifted[o % 8, pl.ds(pl.multiple_of(start + 8 * (o // 8), 8), reach), ln]
                    tap = taps_b[n_taps - 1 - o, :, ln]
                    d_glu = d_glu + jnp.concatenate([tap] * (reach // 8), axis=0) * x
                    prod = gated * x
                    acc = accs[o]
                    for q in range(reach // 8):
                        acc = acc + prod[8 * q:8 * q + 8]
                    out.append(acc)
                d_glu_s[at, ln] = d_glu
                return tuple(out)

            accs = tuple(grad_acc[n_taps - 1 - o, :, ln] for o in range(n_taps))
            accs = lax.fori_loop(first, last, body, accs)
            for o in range(n_taps):
                grad_acc[n_taps - 1 - o, :, ln] = accs[o]

    n_row = rows // reach

    @pl.loop(0, n_row - 1)
    def _(i):
        shift_block(i)

    half = (n_row - 2) // 2
    conv_blocks(0, half)

    @pl.when(end)
    def _():
        hop(0, 0)
        hop(0, 1)

    @pl.when(mid)
    def _():
        low_hop(0)

    conv_blocks(half, n_row - 2)

    @pl.when(s < n_sp - 1)
    def _():
        for i in range(3):
            edge_copy(i).wait_recv()
        per_token = edge_sums_in[...].T[:reach]
        mean_e, inv_e, first_e, second_e = [per_token[:, i:i + 1] for i in range(4)]
        gain_e = gain[...].astype(f32).reshape(1, ch)
        centered = (edge_in[0] - mean_e) * inv_e
        normed = centered * gain_e
        gate = jax.nn.sigmoid(normed)
        d_hat = edge_in[1] * gate * (1.0 + normed * (1.0 - gate)) * gain_e
        ext[pl.ds(rows, reach), :] = inv_e * (d_hat - first_e - centered * second_e)

    @pl.when(s == n_sp - 1)
    def _():
        ext[pl.ds(rows, reach), :] = jnp.zeros((reach, ch), f32)

    shift_block(n_row - 1)
    win = ext[pl.ds(rows, reach), :]
    for o in range(8):
        shifted[o, pl.ds(rows, reach - 8), :] = win[o:o + reach - 8]
    conv_blocks(n_row - 2, n_row)

    for k in range(n_taps):
        g_own[k:k + 1, :] = jnp.sum(grad_acc[k], axis=0, keepdims=True)
    for k in range(n_taps, g_own.shape[0]):
        g_own[k:k + 1, :] = jnp.zeros((1, ch), f32)

    def taps_copy(src, up):
        dst, ss, rs = (g_up, gu_ss, gu_rs) if up else (g_dn, gd_ss, gd_rs)
        to = jnp.clip(z + 1 if up else z - 1, 0, n_z - 1)
        return pltpu.make_async_remote_copy(
            src_ref=src, dst_ref=dst, send_sem=ss, recv_sem=rs,
            device_id=(to * fold + y, t), device_id_type=MESH,
        )

    def taps_pass(up):
        src = g_up if up else g_dn
        out = g_up_out if up else g_dn_out
        taps_copy(g_own, up).wait_recv()
        out[...] = g_own[...] + src[...]
        taps_copy(out, up).start()

    @pl.when(z == 0)
    def _():
        g_up[...] = jnp.zeros_like(g_up)
        taps_copy(g_own, True).start()

    @pl.when(z == n_z - 1)
    def _():
        g_dn[...] = jnp.zeros_like(g_dn)
        taps_copy(g_own, False).start()

    y_start(2, 0, pieces if n_z > 3 else 2)

    @pl.loop(0, n_blk)
    def _(i):
        at = pl.ds(pl.multiple_of(i * blk, blk), blk)
        gate = jax.nn.sigmoid(pg[:, at].astype(f32))
        d_glu = d_glu_s[at, :].T
        out_v[:, at] = (d_glu * gate).astype(jnp.bfloat16)
        out_g[:, at] = (d_glu * (pv[:, at].astype(f32) * gate) * (1.0 - gate)).astype(jnp.bfloat16)

    @pl.when(end)
    def _():
        hop(0, 2)
        hop(0, 3)
        for k in range(1, n_z - 2):
            for h in range(pieces):
                hop(k, h)

    @pl.when(mid)
    def _():
        for k in range(n_z - 2, 0, -1):
            low_hop(k)
        hop(0, 0)
        hop(0, 1)

        @pl.when(2 * z < n_z)
        def _():
            taps_pass(True)

        @pl.when(2 * z >= n_z)
        def _():
            taps_pass(False)

        hop(0, 2)
        hop(0, 3)

    low_end()
    if n_z > 3:
        y_start(n_z - 1, 0, 2)

    @pl.when(end)
    def _():
        for h in range(pieces):
            hop(n_z - 2, h)

    @pl.when(mid)
    def _():
        @pl.when(2 * z < n_z)
        def _():
            taps_pass(False)

        @pl.when(2 * z >= n_z)
        def _():
            taps_pass(True)

        for h in range(pieces):
            hop(1, h)

    @pl.when(z == 0)
    def _():
        taps_copy(g_own, False).wait_recv()

    @pl.when(z == n_z - 1)
    def _():
        taps_copy(g_own, True).wait_recv()

    g_mid[...] = g_own[...] + g_up[...] + g_dn[...]
    gy = pltpu.make_async_remote_copy(
        src_ref=g_mid, dst_ref=g_yin, send_sem=gy_ss, recv_sem=gy_rs,
        device_id=(z * fold + other_y, t), device_id_type=MESH,
    )
    gy.start()
    y_start(n_z - 1, 2, pieces)

    @pl.when(mid)
    def _():
        for k in range(2, n_z - 1):
            for h in range(pieces):
                hop(k, h)

    @pl.when(z < n_z - 1)
    def _():
        taps_copy(g_own, True).wait_send()

    @pl.when(z > 0)
    def _():
        taps_copy(g_own, False).wait_send()

    @pl.when(s > 0)
    def _():
        for i in range(3):
            edge_copy(i).wait_send()

    own = z * fold + y
    low_swap.wait()
    out_w[top:, :] = (term[own, top:, :] + low_y[...]) * scale
    for h in range(pieces):
        y_copies[n_z - 1][h].wait_recv()
        add_into(z, h, got_y, z)

        @pl.when(z > 0)
        def _():
            line_take(z, h, True)

        @pl.when(z < n_z - 1)
        def _():
            line_take(z, h, False)

        out_w[piece(h), :] = term[own, piece(h), :] * scale

    gy.wait()
    out_t[...] = ((g_mid[...] + g_yin[...]) * scale)[:n_taps]

    def all_sent(buf, ss, spare):
        pltpu.make_async_remote_copy(
            src_ref=buf, dst_ref=buf, send_sem=ss, recv_sem=spare,
            device_id=(z * fold + other_y, t), device_id_type=MESH,
        ).wait_send()

    all_sent(low_in.at[pl.ds(0, n_z - 1)], low_ss, ly_rs)
    all_sent(got_y, y_ss, ly_rs)
    all_sent(got_line.at[pl.ds(0, n_z - 1)], line_ss, ly_rs)


def fused(n_sp, n_tp, proj_value, proj_gate, conv_saved, conv_taps, norm_gain, out_weight, cotangent):
    fold = 2
    n_z = n_sp // fold
    rows, width = cotangent.shape
    ch = conv_saved.shape[1]
    n_taps = conv_taps.shape[0]
    part = width // n_sp
    _, top, low = split_rows(ch)
    sums = -(-2 * (rows // 128) // 8) * 8
    dma = pltpu.SemaphoreType.DMA
    V = pltpu.VMEM
    bf = jnp.bfloat16
    vm = pl.BlockSpec(memory_space=pltpu.VMEM)
    hb = pl.BlockSpec(memory_space=pl.ANY)
    grad_value, grad_gate, grad_weight, grad_taps = pl.pallas_call(
        functools.partial(kernel, n_sp, n_tp, fold),
        out_shape=(V((ch, rows), bf), V((ch, rows), bf), V((ch, part), f32), V((n_taps, ch), f32)),
        in_specs=[hb] * 7,
        out_specs=[vm] * 4,
        scratch_shapes=[
            V((ch, rows), bf), V((n_taps, ch), bf), V((ch,), bf),
            V((ch, rows), bf), V((ch, rows), bf), V((ch, width), bf), V((width, rows), bf), dma((7,)),
            V((ch, 128), f32), V((rows, ch), f32), V((rows, ch), f32),
            V((ch, rows), bf), V((ch, rows), f32), V((rows + 32, ch), f32), V((8, rows + 32, ch), f32),
            V((8, rows), f32), V((8, rows), f32),
            V((n_sp, ch, part), f32), V((n_z, top, part), f32), V((n_z + 1, top, part), f32),
            V((n_z + 1, fold, low, part), f32), V((low, part), f32),
            V((sums, 128), f32), V((n_tp - 1, sums, 128), f32),
            V((sums, 128), f32), V((n_tp - 1, sums, 128), f32),
            V((n_taps, 8, ch), f32), *[V((32, ch), f32)] * 7, V((n_taps, 8, ch), f32),
            V((2, 32, ch), f32), V((2, 32, ch), f32), V((8, 128), f32), V((8, 128), f32),
            dma, dma, dma, dma, dma, dma((pieces * n_z,)), dma, dma((pieces * (n_z + 1),)),
            dma, dma((n_z + 1,)), dma, dma, dma((3,)), dma((3,)), *[dma] * 6,
        ],
        compiler_params=pltpu.CompilerParams(
            collective_id=0, has_side_effects=True, vmem_limit_bytes=56 * 1024 * 1024
        ),
    )(
        proj_value.T, proj_gate.T, conv_saved.T, conv_taps, norm_gain, out_weight,
        cotangent.T,
    )
    results = (grad_value, grad_gate, grad_weight, grad_taps)
    grad_value, grad_gate, grad_weight, grad_taps = pl.pallas_call(
        finish,
        out_shape=tuple(jax.ShapeDtypeStruct(r.shape, r.dtype) for r in results),
        in_specs=[vm] * 4,
        out_specs=[hb] * 4,
        scratch_shapes=[dma((4,))],
    )(*[pltpu.with_memory_space_constraint(r, pltpu.VMEM) for r in results])
    return grad_value.T, grad_gate.T, grad_weight, grad_taps


def passed_along(block, axis, distance):
    devices = range(lax.axis_size(axis))
    route = [(i - distance, i) for i in devices if i - distance in devices]
    return lax.ppermute(block, axis, route)


def local(proj_value, proj_gate, conv_saved, conv_taps, norm_gain, out_weight, cotangent):
    model_width = cotangent.shape[1]
    tok_rows = cotangent.shape[0]
    tap_count = conv_taps.shape[0]
    overhang = tap_count - 1
    grad_scale = 1.0 / math.sqrt(tok_rows * lax.axis_size("sp"))
    conv_f = conv_saved.astype(jnp.float32)
    totals = lax.psum((jnp.sum(conv_f, axis=1), jnp.sum(conv_f * conv_f, axis=1)), "tp")
    row_mean = totals[0] / model_width
    row_var = totals[1] / model_width - row_mean * row_mean
    inv_std = lax.rsqrt(row_var + norm_eps)
    centered = (conv_f - row_mean[:, None]) * inv_std[:, None]
    gain_f = norm_gain.astype(jnp.float32)
    normed = centered * gain_f
    gate_norm = jax.nn.sigmoid(normed)
    activated = (normed * gate_norm).astype(jnp.bfloat16)
    contract_rows = (((0,), (0,)), ((), ()))
    whole_term = lax.dot_general(
        cotangent, activated, contract_rows, preferred_element_type=jnp.float32
    )
    shard_grad = lax.psum_scatter(whole_term, "sp", scatter_dimension=0, tiled=True)
    grad_out_weight = shard_grad.T * grad_scale
    d_act = lax.dot_general(
        cotangent, out_weight, (((1,), (1,)), ((), ())), preferred_element_type=jnp.float32
    )
    d_hat = d_act * gate_norm * (1.0 + normed * (1.0 - gate_norm)) * gain_f
    moments = lax.psum((jnp.sum(d_hat, axis=1), jnp.sum(d_hat * centered, axis=1)), "tp")
    first = moments[0] / model_width
    second = moments[1] / model_width
    d_conv = inv_std[:, None] * (d_hat - first[:, None] - centered * second[:, None])
    ahead = passed_along(d_conv[:overhang], "sp", -1)
    extended = jnp.concatenate([d_conv, ahead], axis=0)
    gate_proj = jax.nn.sigmoid(proj_gate.astype(jnp.float32))
    gated = proj_value.astype(jnp.float32) * gate_proj
    taps_f = conv_taps.astype(jnp.float32)
    d_glu = jnp.zeros_like(d_conv)
    tap_rows = []
    for offset in range(tap_count):
        shifted = extended[overhang - offset : overhang - offset + tok_rows]
        d_glu = d_glu + taps_f[offset] * shifted
        tap_rows.append(jnp.sum(gated * shifted, axis=0))
    grad_taps = lax.psum(jnp.stack(tap_rows), "sp") * grad_scale
    grad_value = (d_glu * gate_proj).astype(jnp.bfloat16)
    grad_gate = (d_glu * gated * (1.0 - gate_proj)).astype(jnp.bfloat16)
    return (grad_value, grad_gate, grad_out_weight, grad_taps)


def solution(mesh):
    in_specs = (
        P("sp", "tp"),
        P("sp", "tp"),
        P("sp", "tp"),
        P(None, "tp"),
        P("tp"),
        P("tp", None),
        P("sp", None),
    )
    out_specs = (P("sp", "tp"), P("sp", "tp"), P("tp", "sp"), P(None, "tp"))
    n_sp, n_tp = mesh.shape["sp"], mesh.shape["tp"]

    def step(*args):
        rows, width = args[6].shape
        ch, n_taps = args[2].shape[1], args[3].shape[0]
        small = n_sp % 2 == 0 and 6 <= n_sp <= 8 and width % n_sp == 0 and n_tp > 1
        if small and rows % 128 == 0 and rows >= 128 and ch % 8 == 0 and ch >= 64 and 24 < n_taps <= 31:
            return fused(n_sp, n_tp, *args)
        return local(*args)

    return jax.shard_map(step, mesh=mesh, in_specs=in_specs, out_specs=out_specs, check_vma=False)
```

```python
import functools
import math

import jax
import jax.numpy as jnp
from jax import lax
from jax.experimental import pallas as pl
from jax.experimental.pallas import tpu as pltpu
from jax.sharding import PartitionSpec as P

norm_eps = 1e-05
MESH = pl.DeviceIdType.MESH
f32 = jnp.float32
pieces = 4


def line_order(length):
    rows = []
    for place in range(length):
        side = 1 if 2 * place >= length else -1
        rows.append(sorted(range(length), key=lambda d: (-abs(d - place), -side * (d - place))))
    return rows


def split_rows(ch):
    units = ch * 17 // 20 // 8
    sizes = [8 * (units // pieces + (i < units % pieces)) for i in range(pieces)]
    return sizes, sum(sizes), ch - sum(sizes)


def lookup(table, place):
    value = table[0]
    for i in range(1, len(table)):
        value = jnp.where(place == i, table[i], value)
    return value


def finish(v_in, g_in, w_in, t_in, v_out, g_out, w_out, t_out, ss):
    pairs = [(v_in, v_out), (g_in, g_out), (w_in, w_out), (t_in, t_out)]
    copies = [pltpu.make_async_copy(a, b, ss.at[i]) for i, (a, b) in enumerate(pairs)]
    for c in copies:
        c.start()
    for c in copies:
        c.wait()


def kernel(
    n_sp, n_tp, fold, pv_h, pg_h, conv_h, taps_h, gain_h, weight_h, cot_h,
    out_v, out_g, out_w, out_t,
    conv, taps, gain, pv, pg, weight, cot, in_sems, conv_sems, cot_sems, ready, gain_c, gated_s, d_glu_s, act_t, d_act, ext, shifted, cols, cols2, term, got_y, got_line, low_in, low_y,
    stat, stat_in, mom, mom_in, grad_acc, g_own, g_mid, g_up, g_dn, g_up_out, g_dn_out, g_yin, g_total, taps_b, edge_out, edge_in, edge_sums, edge_sums_in,
    stat_ss, stat_rs, mom_ss, mom_rs, y_ss, y_rs, line_ss, line_rs,
    low_ss, low_rs, ly_ss, ly_rs, edge_ss, edge_rs,
    gu_ss, gu_rs, gd_ss, gd_rs, gy_ss, gy_rs, gt_ss, gt_rs,
):
    s = lax.axis_index("sp")
    t = lax.axis_index("tp")
    n_z = n_sp // fold
    z = s // fold
    y = s % fold
    other_y = 1 - y
    width, rows = cot.shape
    ch = conv.shape[0]
    part = out_w.shape[1]
    n_taps = taps.shape[0]
    scale = 1.0 / math.sqrt(rows * n_sp)
    blk = 128
    n_blk = rows // blk
    sizes, top, low = split_rows(ch)
    end = jnp.logical_or(z == 0, z == n_z - 1)
    mid = jnp.logical_and(z > 0, z < n_z - 1)

    loads = [
        pltpu.make_async_copy(a, b, in_sems.at[i])
        for i, (a, b) in enumerate([
            (weight_h, weight), (pv_h, pv), (pg_h, pg), (gain_h, gain), (taps_h, taps)
        ])
    ]
    conv_loads = [
        pltpu.make_async_copy(
            conv_h.at[:, pl.ds(i * blk, blk)], conv.at[:, pl.ds(i * blk, blk)], conv_sems.at[i]
        )
        for i in range(n_blk)
    ]
    for c in conv_loads:
        c.start()

    barrier = pltpu.get_barrier_semaphore()

    def greet(s_to, t_to):
        pl.semaphore_signal(barrier, inc=1, device_id=(s_to, t_to), device_id_type=MESH)

    for i in range(1, n_tp):
        greet(s, lax.rem(t + i, n_tp))

    @pl.when(y < fold - 1)
    def _():
        greet(s + 1, t)

    @pl.when(z < n_z - 1)
    def _():
        greet(s + fold, t)

        @pl.when(y == fold - 1)
        def _():
            greet(s + 1, t)

    wide_blk = 256 if rows % 256 == 0 else 128
    cot_loads = [
        pltpu.make_async_copy(
            cot_h.at[:, pl.ds(i, wide_blk)], cot.at[:, pl.ds(i, wide_blk)], cot_sems.at[i // wide_blk]
        )
        for i in range(0, rows, wide_blk)
    ]
    loads[3].start()
    loads[0].start()
    for c in cot_loads:
        c.start()

    def put_sums(ref, i, first, second):
        ref[pl.ds(i, 1), :] = jnp.sum(first, axis=0, keepdims=True)
        ref[pl.ds(n_blk + i, 1), :] = jnp.sum(second, axis=0, keepdims=True)

    if stat.shape[0] > 2 * n_blk:
        stat[...] = jnp.zeros_like(stat)
        mom[...] = jnp.zeros_like(mom)

    for i in range(n_blk):
        conv_loads[i].wait()
        c = conv[:, i * blk:(i + 1) * blk].astype(f32)
        put_sums(stat, i, c, c * c)

    first_in_row = jnp.where(y == 0, 1, 0)
    below = jnp.where(z > 0, 1 + first_in_row, 0)
    pl.semaphore_wait(barrier, n_tp - 1 + (1 - first_in_row) + below)

    @pl.when(y > 0)
    def _():
        pl.semaphore_signal(ready, inc=1, device_id=(s - 1, t), device_id_type=MESH)

    @pl.when(z > 0)
    def _():
        pl.semaphore_signal(ready, inc=1, device_id=(s - fold, t), device_id_type=MESH)

    def tp_copies(src, dst, ss, rs):
        return [
            pltpu.make_async_remote_copy(
                src_ref=src, dst_ref=dst.at[i - 1], send_sem=ss, recv_sem=rs,
                device_id=(s, lax.rem(t + i, n_tp)), device_id_type=MESH,
            )
            for i in range(1, n_tp)
        ]

    def tp_wait(dst, ss, rs):
        pltpu.make_async_remote_copy(
            src_ref=dst, dst_ref=dst, send_sem=ss, recv_sem=rs,
            device_id=(s, lax.rem(t + 1, n_tp)), device_id_type=MESH,
        ).wait()

    for c in tp_copies(stat, stat_in, stat_ss, stat_rs):
        c.start()

    reach = 32
    back = jnp.maximum(s - 1, 0)

    def edge_copy(i):
        src, dst = (edge_sums, edge_sums_in) if i == 2 else (edge_out.at[i], edge_in.at[i])
        return pltpu.make_async_remote_copy(
            src_ref=src, dst_ref=dst, send_sem=edge_ss.at[i], recv_sem=edge_rs.at[i],
            device_id=(back, t), device_id_type=MESH,
        )

    def edge_send(i):
        @pl.when(s > 0)
        def _():
            edge_copy(i).start()

    edge_out[0] = conv[:, :blk].astype(f32).T[:reach]
    edge_send(0)
    loads[3].wait()
    gain_c[...] = jnp.broadcast_to(gain[...].astype(f32).reshape(1, ch), (128, ch)).T
    loads[0].wait()
    cot_loads[0].wait()

    d_act[:, :wide_blk] = jnp.dot(weight[...], cot[:, :wide_blk], preferred_element_type=f32)
    edge_out[1] = d_act[:, :blk].T[:reach]
    edge_send(1)

    for i in (1, 2, 4):
        loads[i].start()
    for c in cot_loads[1:]:
        c.wait()
    tp_wait(stat_in, stat_ss, stat_rs)
    total = stat[...]
    for i in range(n_tp - 1):
        total = total + stat_in[i]
    mean = total[:n_blk] / width
    inv = lax.rsqrt(total[n_blk:2 * n_blk] / width - mean * mean + norm_eps)
    for i in range(n_blk):
        cols[0:1, i * blk:(i + 1) * blk] = mean[i:i + 1]
        cols[1:2, i * blk:(i + 1) * blk] = inv[i:i + 1]

    orders = line_order(n_z)
    dest = [lookup([orders[i][k] for i in range(n_z)], z) for k in range(n_z)]

    firsts = [sum(sizes[:h]) for h in range(pieces)]

    def piece(h):
        return pl.ds(firsts[h], sizes[h])

    def y_copy(k, h):
        sem = dest[k] * pieces + h
        return pltpu.make_async_remote_copy(
            src_ref=term.at[dest[k] * fold + other_y, piece(h), :], dst_ref=got_y.at[dest[k], piece(h), :],
            send_sem=y_ss, recv_sem=y_rs.at[sem],
            device_id=(z * fold + other_y, t), device_id_type=MESH,
        )

    y_copies = [[y_copy(k, h) for h in range(pieces)] for k in range(n_z)]

    def y_start(k, first=0, last=pieces):
        for h in range(first, last):
            y_copies[k][h].start()

    def make_term(j, at=slice(None)):
        term[j, at, :] = lax.dot_general(
            act_t[at, :], cot[j * part:(j + 1) * part, :], (((1,), (1,)), ((), ())),
            preferred_element_type=f32,
        )

    lead = dest[0] * fold + other_y
    second = dest[0] * fold + y
    leads = sorted({orders[i][0] * fold + o for i in range(n_z) for o in range(fold)})

    def make_one_of(place, at=slice(None)):
        for j in leads:
            @pl.when(place == j)
            def _():
                make_term(j, at)

    def line_copy(d, h, up):
        slot = d + 1 if up else d
        to = z + 1 if up else z - 1
        to = jnp.clip(to, 0, n_z - 1)
        return pltpu.make_async_remote_copy(
            src_ref=term.at[d * fold + y, piece(h), :], dst_ref=got_line.at[slot, piece(h), :],
            send_sem=line_ss, recv_sem=line_rs.at[slot * pieces + h],
            device_id=(to * fold + y, t), device_id_type=MESH,
        )

    def add_into(d, h, buf, slot):
        own = d * fold + y
        term[own, piece(h), :] = term[own, piece(h), :] + buf[slot, piece(h), :]

    def line_take(d, h, up):
        line_copy(d, h, up).wait_recv()
        add_into(d, h, got_line, d + 1 if up else d)

    def hop(k, h):
        d = dest[k]
        y_copies[k][h].wait_recv()
        add_into(d, h, got_y, d)

        @pl.when(d > z)
        def _():
            @pl.when(z > 0)
            def _():
                line_take(d, h, True)

            line_copy(d, h, True).start()

        @pl.when(d < z)
        def _():
            @pl.when(z < n_z - 1)
            def _():
                line_take(d, h, False)

            line_copy(d, h, False).start()

    def low_copy(d, up):
        slot = d + 1 if up else d
        to = jnp.clip(z + 1 if up else z - 1, 0, n_z - 1)
        return pltpu.make_async_remote_copy(
            src_ref=term.at[pl.ds(d * fold, fold), pl.ds(top, low), :], dst_ref=low_in.at[slot],
            send_sem=low_ss, recv_sem=low_rs.at[slot], device_id=(to * fold + y, t), device_id_type=MESH,
        )

    def low_take(d, up):
        low_copy(d, up).wait_recv()
        at = pl.ds(d * fold, fold)
        term[at, pl.ds(top, low), :] = term[at, pl.ds(top, low), :] + low_in[d + 1 if up else d]

    def low_hop(k):
        d = dest[k]

        @pl.when(d > z)
        def _():
            @pl.when(z > 0)
            def _():
                low_take(d, True)

            low_copy(d, True).start()

        @pl.when(d < z)
        def _():
            @pl.when(z < n_z - 1)
            def _():
                low_take(d, False)

            low_copy(d, False).start()

    low_swap = pltpu.make_async_remote_copy(
        src_ref=term.at[z * fold + other_y, pl.ds(top, low), :], dst_ref=low_y,
        send_sem=ly_ss, recv_sem=ly_rs, device_id=(z * fold + other_y, t), device_id_type=MESH,
    )

    def low_end():
        @pl.when(z > 0)
        def _():
            low_take(z, True)

        @pl.when(z < n_z - 1)
        def _():
            low_take(z, False)

        low_swap.start()

    def activate(at):
        c = conv[at, :].astype(f32)
        gains = jnp.concatenate([gain_c[at, :]] * n_blk, axis=1)
        normed = (c - cols[0:1, :]) * cols[1:2, :] * gains
        act_t[at, :] = (normed * jax.nn.sigmoid(normed)).astype(jnp.bfloat16)

    def lead_piece(h):
        at = slice(firsts[h], firsts[h] + sizes[h])
        activate(at)
        make_one_of(lead, at)
        y_copies[0][h].start()


    @pl.when(jnp.logical_or(y == 0, z < n_z - 1))
    def _():
        pl.semaphore_wait(ready, first_in_row + jnp.where(z < n_z - 1, 1, 0))

    lead_piece(0)
    activate(slice(top, None))
    make_one_of(lead, slice(top, None))
    make_one_of(second, slice(top, None))

    @pl.when(end)
    def _():
        low_hop(0)

    for h in range(1, pieces):
        lead_piece(h)
    make_one_of(second, slice(0, top))

    for j in range(n_sp):
        if j in leads:
            @pl.when(jnp.logical_and(lead != j, second != j))
            def _():
                make_term(j)
        else:
            make_term(j)

    @pl.when(end)
    def _():
        for k in range(1, n_z - 1):
            low_hop(k)

    @pl.loop(1, rows // wide_blk)
    def _(i):
        at = pl.ds(pl.multiple_of(i * wide_blk, wide_blk), wide_blk)
        d_act[:, at] = jnp.dot(weight[...], cot[:, at], preferred_element_type=f32)

    @pl.loop(0, n_blk)
    def _(i):
        at = pl.ds(pl.multiple_of(i * blk, blk), blk)
        c = conv[:, at].astype(f32)
        centered = (c - cols[0:1, at]) * cols[1:2, at]
        normed = centered * gain_c[...]
        gate = jax.nn.sigmoid(normed)
        d_hat = d_act[:, at] * gate * (1.0 + normed * (1.0 - gate)) * gain_c[...]
        d_act[:, at] = d_hat
        put_sums(mom, i, d_hat, d_hat * centered)

    for c in tp_copies(mom, mom_in, mom_ss, mom_rs):
        c.start()
    loads[4].wait()
    for k in range(n_taps):
        taps_b[k] = jnp.broadcast_to(taps[k:k + 1, :].astype(f32), (8, ch))
    grad_acc[...] = jnp.zeros_like(grad_acc)
    loads[1].wait()
    loads[2].wait()

    @pl.loop(0, n_blk)
    def _(i):
        at = pl.ds(pl.multiple_of(i * blk, blk), blk)
        gated_s[at, :] = (pv[:, at].astype(f32) * jax.nn.sigmoid(pg[:, at].astype(f32))).T

    tp_wait(mom_in, mom_ss, mom_rs)
    total = mom[...]
    for i in range(n_tp - 1):
        total = total + mom_in[i]
    total = total / width
    for i in range(n_blk):
        cols2[0:1, i * blk:(i + 1) * blk] = total[i:i + 1]
        cols2[1:2, i * blk:(i + 1) * blk] = total[n_blk + i:n_blk + i + 1]

    edge_sums[...] = jnp.zeros_like(edge_sums)
    edge_sums[0:2, :] = cols[0:2, :blk]
    edge_sums[2:4, :] = cols2[0:2, :blk]
    edge_send(2)
    y_start(1)

    @pl.loop(0, n_blk)
    def _(i):
        at = pl.ds(pl.multiple_of(i * blk, blk), blk)
        c = conv[:, at].astype(f32)
        inv_std = cols[1:2, at]
        centered = (c - cols[0:1, at]) * inv_std
        ext[at, :] = (inv_std * (d_act[:, at] - cols2[0:1, at] - centered * cols2[1:2, at])).T

    def shift_block(i):
        start = pl.multiple_of(i * reach, reach)
        win = ext[pl.ds(start, reach + 8), :]
        for o in range(8):
            shifted[o, pl.ds(start, reach), :] = win[o:o + reach]

    lanes = [(lo, min(128, ch - lo)) for lo in range(0, ch, 128)]

    def conv_blocks(first, last):
        for lo, wide in lanes:
            ln = slice(lo, lo + wide)

            def body(i, accs):
                start = pl.multiple_of(i * reach, reach)
                at = pl.ds(start, reach)
                gated = gated_s[at, ln]
                d_glu = jnp.zeros((reach, wide), f32)
                out = []
                for o in range(n_taps):
                    x = shifted[o % 8, pl.ds(pl.multiple_of(start + 8 * (o // 8), 8), reach), ln]
                    tap = taps_b[n_taps - 1 - o, :, ln]
                    d_glu = d_glu + jnp.concatenate([tap] * (reach // 8), axis=0) * x
                    prod = gated * x
                    acc = accs[o]
                    for q in range(reach // 8):
                        acc = acc + prod[8 * q:8 * q + 8]
                    out.append(acc)
                d_glu_s[at, ln] = d_glu
                return tuple(out)

            accs = tuple(grad_acc[n_taps - 1 - o, :, ln] for o in range(n_taps))
            accs = lax.fori_loop(first, last, body, accs)
            for o in range(n_taps):
                grad_acc[n_taps - 1 - o, :, ln] = accs[o]

    n_row = rows // reach

    @pl.loop(0, n_row - 1)
    def _(i):
        shift_block(i)

    half = (n_row - 2) // 2
    conv_blocks(0, half)

    @pl.when(end)
    def _():
        hop(0, 0)
        hop(0, 1)

    @pl.when(mid)
    def _():
        low_hop(0)

    conv_blocks(half, n_row - 2)

    @pl.when(s < n_sp - 1)
    def _():
        for i in range(3):
            edge_copy(i).wait_recv()
        per_token = edge_sums_in[...].T[:reach]
        mean_e, inv_e, first_e, second_e = [per_token[:, i:i + 1] for i in range(4)]
        gain_e = gain[...].astype(f32).reshape(1, ch)
        centered = (edge_in[0] - mean_e) * inv_e
        normed = centered * gain_e
        gate = jax.nn.sigmoid(normed)
        d_hat = edge_in[1] * gate * (1.0 + normed * (1.0 - gate)) * gain_e
        ext[pl.ds(rows, reach), :] = inv_e * (d_hat - first_e - centered * second_e)

    @pl.when(s == n_sp - 1)
    def _():
        ext[pl.ds(rows, reach), :] = jnp.zeros((reach, ch), f32)

    shift_block(n_row - 1)
    win = ext[pl.ds(rows, reach), :]
    for o in range(8):
        shifted[o, pl.ds(rows, reach - 8), :] = win[o:o + reach - 8]
    conv_blocks(n_row - 2, n_row)

    for k in range(n_taps):
        g_own[k:k + 1, :] = jnp.sum(grad_acc[k], axis=0, keepdims=True)
    for k in range(n_taps, g_own.shape[0]):
        g_own[k:k + 1, :] = jnp.zeros((1, ch), f32)

    def taps_copy(src, up):
        dst, ss, rs = (g_up, gu_ss, gu_rs) if up else (g_dn, gd_ss, gd_rs)
        to = jnp.clip(z + 1 if up else z - 1, 0, n_z - 1)
        return pltpu.make_async_remote_copy(
            src_ref=src, dst_ref=dst, send_sem=ss, recv_sem=rs,
            device_id=(to * fold + y, t), device_id_type=MESH,
        )

    def taps_pass(up):
        src = g_up if up else g_dn
        out = g_up_out if up else g_dn_out
        taps_copy(g_own, up).wait_recv()

        @pl.when(z < n_z - 2 if up else z > 1)
        def _():
            out[...] = g_own[...] + src[...]
            taps_copy(out, up).start()

    @pl.when(z == 0)
    def _():
        taps_copy(g_own, True).start()

    @pl.when(z == n_z - 1)
    def _():
        taps_copy(g_own, False).start()

    y_start(2, 0, pieces if n_z > 3 else 2)

    @pl.loop(0, n_blk)
    def _(i):
        at = pl.ds(pl.multiple_of(i * blk, blk), blk)
        gate = jax.nn.sigmoid(pg[:, at].astype(f32))
        d_glu = d_glu_s[at, :].T
        out_v[:, at] = (d_glu * gate).astype(jnp.bfloat16)
        out_g[:, at] = (d_glu * (pv[:, at].astype(f32) * gate) * (1.0 - gate)).astype(jnp.bfloat16)

    @pl.when(end)
    def _():
        hop(0, 2)
        hop(0, 3)
        for k in range(1, n_z - 2):
            for h in range(pieces):
                hop(k, h)

    @pl.when(mid)
    def _():
        for k in range(n_z - 2, 0, -1):
            low_hop(k)
        hop(0, 0)
        hop(0, 1)

        @pl.when(2 * z < n_z)
        def _():
            taps_pass(True)

        @pl.when(2 * z >= n_z)
        def _():
            taps_pass(False)

        hop(0, 2)
        hop(0, 3)

    low_end()
    gy = pltpu.make_async_remote_copy(
        src_ref=g_mid, dst_ref=g_yin, send_sem=gy_ss, recv_sem=gy_rs,
        device_id=(z * fold + other_y, t), device_id_type=MESH,
    )

    def total_copy(up):
        to = jnp.clip(z + 1 if up else z - 1, 0, n_z - 1)
        return pltpu.make_async_remote_copy(
            src_ref=g_total, dst_ref=g_yin, send_sem=gt_ss.at[int(up)], recv_sem=gt_rs,
            device_id=(to * fold + y, t), device_id_type=MESH,
        )

    y_start(n_z - 1, 0, 1)

    @pl.when(end)
    def _():
        y_start(n_z - 1, 1, pieces)

    @pl.when(end)
    def _():
        for h in range(pieces):
            hop(n_z - 2, h)

    @pl.when(mid)
    def _():
        @pl.when(2 * z < n_z)
        def _():
            taps_pass(False)

        @pl.when(2 * z >= n_z)
        def _():
            taps_pass(True)

        g_mid[...] = g_own[...] + g_up[...] + g_dn[...]
        gy.start()
        y_start(n_z - 1, 1, pieces)
        for h in range(pieces):
            hop(1, h)

    @pl.when(mid)
    def _():
        for k in range(2, n_z - 1):
            for h in range(pieces):
                hop(k, h)

    @pl.when(z < n_z - 2)
    def _():
        taps_copy(g_own, True).wait_send()

    @pl.when(z > 1)
    def _():
        taps_copy(g_own, False).wait_send()

    @pl.when(s > 0)
    def _():
        for i in range(3):
            edge_copy(i).wait_send()

    own = z * fold + y
    low_swap.wait()
    out_w[top:, :] = (term[own, top:, :] + low_y[...]) * scale
    for h in range(pieces):
        if h == 1:
            @pl.when(mid)
            def _():
                gy.wait()
                g_total[...] = g_mid[...] + g_yin[...]

                @pl.when(z == 1)
                def _():
                    total_copy(False).start()

                @pl.when(z == n_z - 2)
                def _():
                    total_copy(True).start()

        y_copies[n_z - 1][h].wait_recv()
        add_into(z, h, got_y, z)

        @pl.when(z > 0)
        def _():
            line_take(z, h, True)

        @pl.when(z < n_z - 1)
        def _():
            line_take(z, h, False)

        out_w[piece(h), :] = term[own, piece(h), :] * scale

    @pl.when(end)
    def _():
        total_copy(True).wait_recv()
        out_t[...] = (g_yin[...] * scale)[:n_taps]

    @pl.when(mid)
    def _():
        out_t[...] = (g_total[...] * scale)[:n_taps]

        @pl.when(z == 1)
        def _():
            total_copy(False).wait_send()

        @pl.when(z == n_z - 2)
        def _():
            total_copy(True).wait_send()


    def all_sent(buf, ss, spare):
        pltpu.make_async_remote_copy(
            src_ref=buf, dst_ref=buf, send_sem=ss, recv_sem=spare,
            device_id=(z * fold + other_y, t), device_id_type=MESH,
        ).wait_send()

    all_sent(low_in.at[pl.ds(0, n_z - 1)], low_ss, ly_rs)
    all_sent(got_y, y_ss, ly_rs)
    all_sent(got_line.at[pl.ds(0, n_z - 1)], line_ss, ly_rs)


def fused(n_sp, n_tp, proj_value, proj_gate, conv_saved, conv_taps, norm_gain, out_weight, cotangent):
    fold = 2
    n_z = n_sp // fold
    rows, width = cotangent.shape
    ch = conv_saved.shape[1]
    n_taps = conv_taps.shape[0]
    part = width // n_sp
    _, top, low = split_rows(ch)
    sums = -(-2 * (rows // 128) // 8) * 8
    dma = pltpu.SemaphoreType.DMA
    V = pltpu.VMEM
    bf = jnp.bfloat16
    vm = pl.BlockSpec(memory_space=pltpu.VMEM)
    hb = pl.BlockSpec(memory_space=pl.ANY)
    grad_value, grad_gate, grad_weight, grad_taps = pl.pallas_call(
        functools.partial(kernel, n_sp, n_tp, fold),
        out_shape=(V((ch, rows), bf), V((ch, rows), bf), V((ch, part), f32), V((n_taps, ch), f32)),
        in_specs=[hb] * 7,
        out_specs=[vm] * 4,
        scratch_shapes=[
            V((ch, rows), bf), V((n_taps, ch), bf), V((ch,), bf),
            V((ch, rows), bf), V((ch, rows), bf), V((ch, width), bf), V((width, rows), bf), dma((5,)), dma((rows // 128,)), dma((rows // (256 if rows % 256 == 0 else 128),)), pltpu.SemaphoreType.REGULAR,
            V((ch, 128), f32), V((rows, ch), f32), V((rows, ch), f32),
            V((ch, rows), bf), V((ch, rows), f32), V((rows + 32, ch), f32), V((8, rows + 32, ch), f32),
            V((8, rows), f32), V((8, rows), f32),
            V((n_sp, ch, part), f32), V((n_z, top, part), f32), V((n_z + 1, top, part), f32),
            V((n_z + 1, fold, low, part), f32), V((low, part), f32),
            V((sums, 128), f32), V((n_tp - 1, sums, 128), f32),
            V((sums, 128), f32), V((n_tp - 1, sums, 128), f32),
            V((n_taps, 8, ch), f32), *[V((32, ch), f32)] * 8, V((n_taps, 8, ch), f32),
            V((2, 32, ch), f32), V((2, 32, ch), f32), V((8, 128), f32), V((8, 128), f32),
            dma, dma, dma, dma, dma, dma((pieces * n_z,)), dma, dma((pieces * (n_z + 1),)),
            dma, dma((n_z + 1,)), dma, dma, dma((3,)), dma((3,)), *[dma] * 6, dma((2,)), dma,
        ],
        compiler_params=pltpu.CompilerParams(
            collective_id=0, has_side_effects=True, vmem_limit_bytes=56 * 1024 * 1024
        ),
    )(
        proj_value.T, proj_gate.T, conv_saved.T, conv_taps, norm_gain, out_weight,
        cotangent.T,
    )
    results = (grad_value, grad_gate, grad_weight, grad_taps)
    grad_value, grad_gate, grad_weight, grad_taps = pl.pallas_call(
        finish,
        out_shape=tuple(jax.ShapeDtypeStruct(r.shape, r.dtype) for r in results),
        in_specs=[vm] * 4,
        out_specs=[hb] * 4,
        scratch_shapes=[dma((4,))],
    )(*[pltpu.with_memory_space_constraint(r, pltpu.VMEM) for r in results])
    return grad_value.T, grad_gate.T, grad_weight, grad_taps


def passed_along(block, axis, distance):
    devices = range(lax.axis_size(axis))
    route = [(i - distance, i) for i in devices if i - distance in devices]
    return lax.ppermute(block, axis, route)


def local(proj_value, proj_gate, conv_saved, conv_taps, norm_gain, out_weight, cotangent):
    model_width = cotangent.shape[1]
    tok_rows = cotangent.shape[0]
    tap_count = conv_taps.shape[0]
    overhang = tap_count - 1
    grad_scale = 1.0 / math.sqrt(tok_rows * lax.axis_size("sp"))
    conv_f = conv_saved.astype(jnp.float32)
    totals = lax.psum((jnp.sum(conv_f, axis=1), jnp.sum(conv_f * conv_f, axis=1)), "tp")
    row_mean = totals[0] / model_width
    row_var = totals[1] / model_width - row_mean * row_mean
    inv_std = lax.rsqrt(row_var + norm_eps)
    centered = (conv_f - row_mean[:, None]) * inv_std[:, None]
    gain_f = norm_gain.astype(jnp.float32)
    normed = centered * gain_f
    gate_norm = jax.nn.sigmoid(normed)
    activated = (normed * gate_norm).astype(jnp.bfloat16)
    contract_rows = (((0,), (0,)), ((), ()))
    whole_term = lax.dot_general(
        cotangent, activated, contract_rows, preferred_element_type=jnp.float32
    )
    shard_grad = lax.psum_scatter(whole_term, "sp", scatter_dimension=0, tiled=True)
    grad_out_weight = shard_grad.T * grad_scale
    d_act = lax.dot_general(
        cotangent, out_weight, (((1,), (1,)), ((), ())), preferred_element_type=jnp.float32
    )
    d_hat = d_act * gate_norm * (1.0 + normed * (1.0 - gate_norm)) * gain_f
    moments = lax.psum((jnp.sum(d_hat, axis=1), jnp.sum(d_hat * centered, axis=1)), "tp")
    first = moments[0] / model_width
    second = moments[1] / model_width
    d_conv = inv_std[:, None] * (d_hat - first[:, None] - centered * second[:, None])
    ahead = passed_along(d_conv[:overhang], "sp", -1)
    extended = jnp.concatenate([d_conv, ahead], axis=0)
    gate_proj = jax.nn.sigmoid(proj_gate.astype(jnp.float32))
    gated = proj_value.astype(jnp.float32) * gate_proj
    taps_f = conv_taps.astype(jnp.float32)
    d_glu = jnp.zeros_like(d_conv)
    tap_rows = []
    for offset in range(tap_count):
        shifted = extended[overhang - offset : overhang - offset + tok_rows]
        d_glu = d_glu + taps_f[offset] * shifted
        tap_rows.append(jnp.sum(gated * shifted, axis=0))
    grad_taps = lax.psum(jnp.stack(tap_rows), "sp") * grad_scale
    grad_value = (d_glu * gate_proj).astype(jnp.bfloat16)
    grad_gate = (d_glu * gated * (1.0 - gate_proj)).astype(jnp.bfloat16)
    return (grad_value, grad_gate, grad_out_weight, grad_taps)


def solution(mesh):
    in_specs = (
        P("sp", "tp"),
        P("sp", "tp"),
        P("sp", "tp"),
        P(None, "tp"),
        P("tp"),
        P("tp", None),
        P("sp", None),
    )
    out_specs = (P("sp", "tp"), P("sp", "tp"), P("tp", "sp"), P(None, "tp"))
    n_sp, n_tp = mesh.shape["sp"], mesh.shape["tp"]

    def step(*args):
        rows, width = args[6].shape
        ch, n_taps = args[2].shape[1], args[3].shape[0]
        small = n_sp % 2 == 0 and 6 <= n_sp <= 8 and width % n_sp == 0 and n_tp > 1
        if small and rows % 128 == 0 and rows >= 128 and ch % 8 == 0 and ch >= 64 and 24 < n_taps <= 31:
            return fused(n_sp, n_tp, *args)
        return local(*args)

    return jax.shard_map(step, mesh=mesh, in_specs=in_specs, out_specs=out_specs, check_vma=False)
```

```python
import functools
import math

import jax
import jax.numpy as jnp
from jax import lax
from jax.experimental import pallas as pl
from jax.experimental.pallas import tpu as pltpu
from jax.sharding import PartitionSpec as P

norm_eps = 1e-05
MESH = pl.DeviceIdType.MESH
f32 = jnp.float32
pieces = 4


def line_order(length):
    rows = []
    for place in range(length):
        side = 1 if 2 * place >= length else -1
        rows.append(sorted(range(length), key=lambda d: (-abs(d - place), -side * (d - place))))
    return rows


def split_rows(ch):
    low, wide = ch // 6 // 8 * 8, ch // 9 * 2 // 8 * 8
    units = (ch - wide) // 8
    sizes = [8 * (units // (pieces - 1) + (i < units % (pieces - 1))) for i in range(pieces - 1)]
    return sizes + [wide - low], low, wide


def lookup(table, place):
    value = table[0]
    for i in range(1, len(table)):
        value = jnp.where(place == i, table[i], value)
    return value


def finish(v_in, g_in, w_in, t_in, v_out, g_out, w_out, t_out, ss):
    pairs = [(v_in, v_out), (g_in, g_out), (w_in, w_out), (t_in, t_out)]
    copies = [pltpu.make_async_copy(a, b, ss.at[i]) for i, (a, b) in enumerate(pairs)]
    for c in copies:
        c.start()
    for c in copies:
        c.wait()


def kernel(
    n_sp, n_tp, fold, pv_h, pg_h, conv_h, taps_h, gain_h, weight_h, cot_h,
    out_v, out_g, out_w, out_t,
    conv, taps, gain, pv, pg, weight, cot, in_sems, conv_sems, cot_sems, ready, gain_c, gated_s, d_glu_s, act_t, d_act, ext, shifted, cols, cols2, term, got_y, got_line, low_in, low_y,
    stat, stat_in, mom, mom_in, grad_acc, g_own, g_mid, g_up, g_dn, g_up_out, g_dn_out, g_yin, g_total, taps_b, edge_out, edge_in, edge_sums, edge_sums_in, wide_in, wide_y,
    stat_ss, stat_rs, mom_ss, mom_rs, y_ss, y_rs, line_ss, line_rs,
    low_ss, low_rs, wide_ss, wide_rs, ly_ss, ly_rs, edge_ss, edge_rs,
    gu_ss, gu_rs, gd_ss, gd_rs, gy_ss, gy_rs, gt_ss, gt_rs,
):
    s = lax.axis_index("sp")
    t = lax.axis_index("tp")
    n_z = n_sp // fold
    z = s // fold
    y = s % fold
    other_y = 1 - y
    width, rows = cot.shape
    ch = conv.shape[0]
    part = out_w.shape[1]
    n_taps = taps.shape[0]
    scale = 1.0 / math.sqrt(rows * n_sp)
    blk = 128
    n_blk = rows // blk
    sizes, low, wide = split_rows(ch)
    base, top, swing = ch - wide, ch - low, wide - low
    last = n_z - 1
    end = jnp.logical_or(z == 0, z == n_z - 1)
    mid = jnp.logical_and(z > 0, z < n_z - 1)

    loads = [
        pltpu.make_async_copy(a, b, in_sems.at[i])
        for i, (a, b) in enumerate([
            (weight_h, weight), (pv_h, pv), (pg_h, pg), (gain_h, gain), (taps_h, taps)
        ])
    ]
    conv_loads = [
        pltpu.make_async_copy(
            conv_h.at[:, pl.ds(i * blk, blk)], conv.at[:, pl.ds(i * blk, blk)], conv_sems.at[i]
        )
        for i in range(n_blk)
    ]
    for c in conv_loads:
        c.start()

    barrier = pltpu.get_barrier_semaphore()

    def greet(s_to, t_to):
        pl.semaphore_signal(barrier, inc=1, device_id=(s_to, t_to), device_id_type=MESH)

    for i in range(1, n_tp):
        greet(s, lax.rem(t + i, n_tp))

    @pl.when(y < fold - 1)
    def _():
        greet(s + 1, t)

    @pl.when(z < n_z - 1)
    def _():
        greet(s + fold, t)

        @pl.when(y == fold - 1)
        def _():
            greet(s + 1, t)

    wide_blk = 256 if rows % 256 == 0 else 128
    cot_loads = [
        pltpu.make_async_copy(
            cot_h.at[:, pl.ds(i, wide_blk)], cot.at[:, pl.ds(i, wide_blk)], cot_sems.at[i // wide_blk]
        )
        for i in range(0, rows, wide_blk)
    ]
    loads[3].start()
    loads[0].start()
    for c in cot_loads:
        c.start()

    def put_sums(ref, i, first, second):
        ref[pl.ds(i, 1), :] = jnp.sum(first, axis=0, keepdims=True)
        ref[pl.ds(n_blk + i, 1), :] = jnp.sum(second, axis=0, keepdims=True)

    if stat.shape[0] > 2 * n_blk:
        stat[...] = jnp.zeros_like(stat)
        mom[...] = jnp.zeros_like(mom)

    for i in range(n_blk):
        conv_loads[i].wait()
        c = conv[:, i * blk:(i + 1) * blk].astype(f32)
        put_sums(stat, i, c, c * c)

    first_in_row = jnp.where(y == 0, 1, 0)
    below = jnp.where(z > 0, 1 + first_in_row, 0)
    pl.semaphore_wait(barrier, n_tp - 1 + (1 - first_in_row) + below)

    @pl.when(y > 0)
    def _():
        pl.semaphore_signal(ready, inc=1, device_id=(s - 1, t), device_id_type=MESH)

    @pl.when(z > 0)
    def _():
        pl.semaphore_signal(ready, inc=1, device_id=(s - fold, t), device_id_type=MESH)

    def tp_copies(src, dst, ss, rs):
        return [
            pltpu.make_async_remote_copy(
                src_ref=src, dst_ref=dst.at[i - 1], send_sem=ss, recv_sem=rs,
                device_id=(s, lax.rem(t + i, n_tp)), device_id_type=MESH,
            )
            for i in range(1, n_tp)
        ]

    def tp_wait(dst, ss, rs):
        pltpu.make_async_remote_copy(
            src_ref=dst, dst_ref=dst, send_sem=ss, recv_sem=rs,
            device_id=(s, lax.rem(t + 1, n_tp)), device_id_type=MESH,
        ).wait()

    for c in tp_copies(stat, stat_in, stat_ss, stat_rs):
        c.start()

    reach = 32
    back = jnp.maximum(s - 1, 0)

    def edge_copy(i):
        src, dst = (edge_sums, edge_sums_in) if i == 2 else (edge_out.at[i], edge_in.at[i])
        return pltpu.make_async_remote_copy(
            src_ref=src, dst_ref=dst, send_sem=edge_ss.at[i], recv_sem=edge_rs.at[i],
            device_id=(back, t), device_id_type=MESH,
        )

    def edge_send(i):
        @pl.when(s > 0)
        def _():
            edge_copy(i).start()

    edge_out[0] = conv[:, :blk].astype(f32).T[:reach]
    edge_send(0)
    loads[3].wait()
    gain_c[...] = jnp.broadcast_to(gain[...].astype(f32).reshape(1, ch), (128, ch)).T
    loads[0].wait()
    cot_loads[0].wait()

    d_act[:, :wide_blk] = jnp.dot(weight[...], cot[:, :wide_blk], preferred_element_type=f32)
    edge_out[1] = d_act[:, :blk].T[:reach]
    edge_send(1)

    for i in (1, 2, 4):
        loads[i].start()
    for c in cot_loads[1:]:
        c.wait()
    tp_wait(stat_in, stat_ss, stat_rs)
    total = stat[...]
    for i in range(n_tp - 1):
        total = total + stat_in[i]
    mean = total[:n_blk] / width
    inv = lax.rsqrt(total[n_blk:2 * n_blk] / width - mean * mean + norm_eps)
    for i in range(n_blk):
        cols[0:1, i * blk:(i + 1) * blk] = mean[i:i + 1]
        cols[1:2, i * blk:(i + 1) * blk] = inv[i:i + 1]

    orders = line_order(n_z)
    dest = [lookup([orders[i][k] for i in range(n_z)], z) for k in range(n_z)]

    firsts = [sum(sizes[:h]) for h in range(pieces)]

    def piece(h):
        return pl.ds(firsts[h], sizes[h])

    def y_copy(k, h):
        sem = dest[k] * pieces + h
        return pltpu.make_async_remote_copy(
            src_ref=term.at[dest[k] * fold + other_y, piece(h), :], dst_ref=got_y.at[dest[k], piece(h), :],
            send_sem=y_ss.at[int(h == pieces - 1)], recv_sem=y_rs.at[sem],
            device_id=(z * fold + other_y, t), device_id_type=MESH,
        )

    y_copies = [[y_copy(k, h) for h in range(pieces)] for k in range(n_z)]

    def y_start(k, first=0, past=pieces):
        for h in range(first, past):
            if h < pieces - 1:
                y_copies[k][h].start()
            else:
                @pl.when(dest[k] != last)
                def _():
                    y_copies[k][h].start()

    def make_term(j, at=slice(None)):
        term[j, at, :] = lax.dot_general(
            act_t[at, :], cot[j * part:(j + 1) * part, :], (((1,), (1,)), ((), ())),
            preferred_element_type=f32,
        )

    lead = dest[0] * fold + other_y
    second = dest[0] * fold + y
    leads = sorted({orders[i][0] * fold + o for i in range(n_z) for o in range(fold)})

    def make_one_of(place, at=slice(None)):
        for j in leads:
            @pl.when(place == j)
            def _():
                make_term(j, at)

    def line_copy(d, h, up):
        slot = d + 1 if up else d
        to = z + 1 if up else z - 1
        to = jnp.clip(to, 0, n_z - 1)
        return pltpu.make_async_remote_copy(
            src_ref=term.at[d * fold + y, piece(h), :], dst_ref=got_line.at[slot, piece(h), :],
            send_sem=line_ss.at[int(h == pieces - 1)], recv_sem=line_rs.at[slot * pieces + h],
            device_id=(to * fold + y, t), device_id_type=MESH,
        )

    def add_into(d, h, buf, slot):
        own = d * fold + y
        term[own, piece(h), :] = term[own, piece(h), :] + buf[slot, piece(h), :]

    def line_take(d, h, up):
        line_copy(d, h, up).wait_recv()
        add_into(d, h, got_line, d + 1 if up else d)

    def hop_always(k, h):
        d = dest[k]
        y_copies[k][h].wait_recv()
        add_into(d, h, got_y, d)

        @pl.when(d > z)
        def _():
            @pl.when(z > 0)
            def _():
                line_take(d, h, True)

            line_copy(d, h, True).start()

        @pl.when(d < z)
        def _():
            @pl.when(z < n_z - 1)
            def _():
                line_take(d, h, False)

            line_copy(d, h, False).start()

    def hop(k, h):
        if h < pieces - 1:
            hop_always(k, h)
        else:
            @pl.when(dest[k] != last)
            def _():
                hop_always(k, h)

    def low_copy(d, up):
        slot = d + 1 if up else d
        to = jnp.clip(z + 1 if up else z - 1, 0, n_z - 1)
        return pltpu.make_async_remote_copy(
            src_ref=term.at[pl.ds(d * fold, fold), pl.ds(top, low), :], dst_ref=low_in.at[slot],
            send_sem=low_ss, recv_sem=low_rs.at[slot], device_id=(to * fold + y, t), device_id_type=MESH,
        )

    def low_take(d, up):
        low_copy(d, up).wait_recv()
        at = pl.ds(d * fold, fold)
        term[at, pl.ds(top, low), :] = term[at, pl.ds(top, low), :] + low_in[d + 1 if up else d]

    wide_copy = pltpu.make_async_remote_copy(
        src_ref=term.at[pl.ds(last * fold, fold), pl.ds(base, wide), :], dst_ref=wide_in,
        send_sem=wide_ss, recv_sem=wide_rs,
        device_id=(jnp.clip(z + 1, 0, last) * fold + y, t), device_id_type=MESH,
    )

    def wide_take():
        wide_copy.wait_recv()
        at = slice(last * fold, n_sp)
        term[at, base:, :] = term[at, base:, :] + wide_in[...]

    def low_hop(k):
        d = dest[k]

        @pl.when(d == last)
        def _():
            @pl.when(z > 0)
            def _():
                wide_take()

            wide_copy.start()

        @pl.when(jnp.logical_and(d > z, d < last))
        def _():
            @pl.when(z > 0)
            def _():
                low_take(d, True)

            low_copy(d, True).start()

        @pl.when(d < z)
        def _():
            @pl.when(z < last)
            def _():
                low_take(d, False)

            low_copy(d, False).start()

    def swap_copy(first, count, into):
        return pltpu.make_async_remote_copy(
            src_ref=term.at[z * fold + other_y, pl.ds(first, count), :], dst_ref=into,
            send_sem=ly_ss, recv_sem=ly_rs, device_id=(z * fold + other_y, t), device_id_type=MESH,
        )

    def low_end():
        @pl.when(z < last)
        def _():
            @pl.when(z > 0)
            def _():
                low_take(z, True)

            low_take(z, False)
            swap_copy(top, low, low_y).start()

        @pl.when(z == last)
        def _():
            wide_take()
            swap_copy(base, wide, wide_y).start()

    def activate(at):
        c = conv[at, :].astype(f32)
        gains = jnp.concatenate([gain_c[at, :]] * n_blk, axis=1)
        normed = (c - cols[0:1, :]) * cols[1:2, :] * gains
        act_t[at, :] = (normed * jax.nn.sigmoid(normed)).astype(jnp.bfloat16)

    def lead_piece(h):
        at = slice(firsts[h], firsts[h] + sizes[h])
        activate(at)
        make_one_of(lead, at)
        y_start(0, h, h + 1)


    @pl.when(jnp.logical_or(y == 0, z < n_z - 1))
    def _():
        pl.semaphore_wait(ready, first_in_row + jnp.where(z < n_z - 1, 1, 0))

    @pl.when(z < n_z - 1)
    def _():
        lead_piece(0)

    activate(slice(base, None))
    make_one_of(lead, slice(base, None))
    make_one_of(second, slice(base, None))

    @pl.when(end)
    def _():
        low_hop(0)

    @pl.when(z == n_z - 1)
    def _():
        lead_piece(0)

    for h in range(1, pieces - 1):
        lead_piece(h)
    y_start(0, pieces - 1)
    make_one_of(second, slice(0, base))

    for j in range(n_sp):
        if j in leads:
            @pl.when(jnp.logical_and(lead != j, second != j))
            def _():
                make_term(j)
        else:
            make_term(j)

    @pl.when(end)
    def _():
        for k in range(1, n_z - 1):
            low_hop(k)

    @pl.loop(1, rows // wide_blk)
    def _(i):
        at = pl.ds(pl.multiple_of(i * wide_blk, wide_blk), wide_blk)
        d_act[:, at] = jnp.dot(weight[...], cot[:, at], preferred_element_type=f32)

    @pl.loop(0, n_blk)
    def _(i):
        at = pl.ds(pl.multiple_of(i * blk, blk), blk)
        c = conv[:, at].astype(f32)
        centered = (c - cols[0:1, at]) * cols[1:2, at]
        normed = centered * gain_c[...]
        gate = jax.nn.sigmoid(normed)
        d_hat = d_act[:, at] * gate * (1.0 + normed * (1.0 - gate)) * gain_c[...]
        d_act[:, at] = d_hat
        put_sums(mom, i, d_hat, d_hat * centered)

    for c in tp_copies(mom, mom_in, mom_ss, mom_rs):
        c.start()
    loads[4].wait()
    for k in range(n_taps):
        taps_b[k] = jnp.broadcast_to(taps[k:k + 1, :].astype(f32), (8, ch))
    grad_acc[...] = jnp.zeros_like(grad_acc)
    loads[1].wait()
    loads[2].wait()

    @pl.loop(0, n_blk)
    def _(i):
        at = pl.ds(pl.multiple_of(i * blk, blk), blk)
        gated_s[at, :] = (pv[:, at].astype(f32) * jax.nn.sigmoid(pg[:, at].astype(f32))).T

    tp_wait(mom_in, mom_ss, mom_rs)
    total = mom[...]
    for i in range(n_tp - 1):
        total = total + mom_in[i]
    total = total / width
    for i in range(n_blk):
        cols2[0:1, i * blk:(i + 1) * blk] = total[i:i + 1]
        cols2[1:2, i * blk:(i + 1) * blk] = total[n_blk + i:n_blk + i + 1]

    edge_sums[...] = jnp.zeros_like(edge_sums)
    edge_sums[0:2, :] = cols[0:2, :blk]
    edge_sums[2:4, :] = cols2[0:2, :blk]
    edge_send(2)
    y_start(1)

    @pl.loop(0, n_blk)
    def _(i):
        at = pl.ds(pl.multiple_of(i * blk, blk), blk)
        c = conv[:, at].astype(f32)
        inv_std = cols[1:2, at]
        centered = (c - cols[0:1, at]) * inv_std
        ext[at, :] = (inv_std * (d_act[:, at] - cols2[0:1, at] - centered * cols2[1:2, at])).T

    def shift_block(i):
        start = pl.multiple_of(i * reach, reach)
        win = ext[pl.ds(start, reach + 8), :]
        for o in range(8):
            shifted[o, pl.ds(start, reach), :] = win[o:o + reach]

    lanes = [(lo, min(128, ch - lo)) for lo in range(0, ch, 128)]

    def conv_blocks(first, last):
        for lo, wide in lanes:
            ln = slice(lo, lo + wide)

            def body(i, accs):
                start = pl.multiple_of(i * reach, reach)
                at = pl.ds(start, reach)
                gated = gated_s[at, ln]
                d_glu = jnp.zeros((reach, wide), f32)
                out = []
                for o in range(n_taps):
                    x = shifted[o % 8, pl.ds(pl.multiple_of(start + 8 * (o // 8), 8), reach), ln]
                    tap = taps_b[n_taps - 1 - o, :, ln]
                    d_glu = d_glu + jnp.concatenate([tap] * (reach // 8), axis=0) * x
                    prod = gated * x
                    acc = accs[o]
                    for q in range(reach // 8):
                        acc = acc + prod[8 * q:8 * q + 8]
                    out.append(acc)
                d_glu_s[at, ln] = d_glu
                return tuple(out)

            accs = tuple(grad_acc[n_taps - 1 - o, :, ln] for o in range(n_taps))
            accs = lax.fori_loop(first, last, body, accs)
            for o in range(n_taps):
                grad_acc[n_taps - 1 - o, :, ln] = accs[o]

    n_row = rows // reach

    @pl.loop(0, n_row - 1)
    def _(i):
        shift_block(i)

    half = (n_row - 2) // 2
    conv_blocks(0, half)

    @pl.when(end)
    def _():
        hop(0, 0)
        hop(0, 1)

    @pl.when(mid)
    def _():
        low_hop(0)

    conv_blocks(half, n_row - 2)

    @pl.when(s < n_sp - 1)
    def _():
        for i in range(3):
            edge_copy(i).wait_recv()
        per_token = edge_sums_in[...].T[:reach]
        mean_e, inv_e, first_e, second_e = [per_token[:, i:i + 1] for i in range(4)]
        gain_e = gain[...].astype(f32).reshape(1, ch)
        centered = (edge_in[0] - mean_e) * inv_e
        normed = centered * gain_e
        gate = jax.nn.sigmoid(normed)
        d_hat = edge_in[1] * gate * (1.0 + normed * (1.0 - gate)) * gain_e
        ext[pl.ds(rows, reach), :] = inv_e * (d_hat - first_e - centered * second_e)

    @pl.when(s == n_sp - 1)
    def _():
        ext[pl.ds(rows, reach), :] = jnp.zeros((reach, ch), f32)

    shift_block(n_row - 1)
    win = ext[pl.ds(rows, reach), :]
    for o in range(8):
        shifted[o, pl.ds(rows, reach - 8), :] = win[o:o + reach - 8]
    conv_blocks(n_row - 2, n_row)

    for k in range(n_taps):
        g_own[k:k + 1, :] = jnp.sum(grad_acc[k], axis=0, keepdims=True)
    for k in range(n_taps, g_own.shape[0]):
        g_own[k:k + 1, :] = jnp.zeros((1, ch), f32)

    def taps_copy(src, up):
        dst, ss, rs = (g_up, gu_ss, gu_rs) if up else (g_dn, gd_ss, gd_rs)
        to = jnp.clip(z + 1 if up else z - 1, 0, n_z - 1)
        return pltpu.make_async_remote_copy(
            src_ref=src, dst_ref=dst, send_sem=ss, recv_sem=rs,
            device_id=(to * fold + y, t), device_id_type=MESH,
        )

    def taps_pass(up):
        src = g_up if up else g_dn
        out = g_up_out if up else g_dn_out
        taps_copy(g_own, up).wait_recv()

        @pl.when(z < n_z - 2 if up else z > 1)
        def _():
            out[...] = g_own[...] + src[...]
            taps_copy(out, up).start()

    @pl.when(z == 0)
    def _():
        taps_copy(g_own, True).start()

    @pl.when(z == n_z - 1)
    def _():
        taps_copy(g_own, False).start()

    y_start(2, 0, pieces if n_z > 3 else 2)

    @pl.loop(0, n_blk)
    def _(i):
        at = pl.ds(pl.multiple_of(i * blk, blk), blk)
        gate = jax.nn.sigmoid(pg[:, at].astype(f32))
        d_glu = d_glu_s[at, :].T
        out_v[:, at] = (d_glu * gate).astype(jnp.bfloat16)
        out_g[:, at] = (d_glu * (pv[:, at].astype(f32) * gate) * (1.0 - gate)).astype(jnp.bfloat16)

    @pl.when(end)
    def _():
        hop(0, 2)
        hop(0, 3)
        for k in range(1, n_z - 2):
            for h in range(pieces):
                hop(k, h)

    @pl.when(mid)
    def _():
        for k in range(n_z - 2, 0, -1):
            low_hop(k)
        hop(0, 0)
        hop(0, 1)

        @pl.when(2 * z < n_z)
        def _():
            taps_pass(True)

        @pl.when(2 * z >= n_z)
        def _():
            taps_pass(False)

        hop(0, 2)
        hop(0, 3)

    low_end()
    gy = pltpu.make_async_remote_copy(
        src_ref=g_mid, dst_ref=g_yin, send_sem=gy_ss, recv_sem=gy_rs,
        device_id=(z * fold + other_y, t), device_id_type=MESH,
    )

    def total_copy(up):
        to = jnp.clip(z + 1 if up else z - 1, 0, n_z - 1)
        return pltpu.make_async_remote_copy(
            src_ref=g_total, dst_ref=g_yin, send_sem=gt_ss.at[int(up)], recv_sem=gt_rs,
            device_id=(to * fold + y, t), device_id_type=MESH,
        )

    y_start(n_z - 1, 0, 1)

    @pl.when(end)
    def _():
        y_start(n_z - 1, 1, pieces)

    @pl.when(end)
    def _():
        for h in range(pieces):
            hop(n_z - 2, h)

    @pl.when(mid)
    def _():
        @pl.when(2 * z < n_z)
        def _():
            taps_pass(False)

        @pl.when(2 * z >= n_z)
        def _():
            taps_pass(True)

        g_mid[...] = g_own[...] + g_up[...] + g_dn[...]
        gy.start()
        y_start(n_z - 1, 1, pieces)
        later = [(k, h) for k in range(1, n_z - 1) for h in range(pieces)]
        for k, h in sorted(later, key=lambda p: (p[1] + 2 * p[0], p[0])):
            hop(k, h)


    @pl.when(z < n_z - 2)
    def _():
        taps_copy(g_own, True).wait_send()

    @pl.when(z > 1)
    def _():
        taps_copy(g_own, False).wait_send()

    @pl.when(s > 0)
    def _():
        for i in range(3):
            edge_copy(i).wait_send()

    own = z * fold + y

    @pl.when(z < last)
    def _():
        swap_copy(top, low, low_y).wait()
        out_w[top:, :] = (term[own, top:, :] + low_y[...]) * scale

    @pl.when(z == last)
    def _():
        swap_copy(base, wide, wide_y).wait()
        out_w[base:, :] = (term[own, base:, :] + wide_y[...]) * scale

    def own_piece(h):
        y_copies[last][h].wait_recv()
        add_into(z, h, got_y, z)

        @pl.when(z > 0)
        def _():
            line_take(z, h, True)

        @pl.when(z < last)
        def _():
            line_take(z, h, False)

        out_w[piece(h), :] = term[own, piece(h), :] * scale

    @pl.when(mid)
    def _():
        gy.wait()
        g_total[...] = g_mid[...] + g_yin[...]

        @pl.when(z == 1)
        def _():
            total_copy(False).start()

        @pl.when(z == n_z - 2)
        def _():
            total_copy(True).start()

    for h in range(pieces - 1):
        own_piece(h)

    @pl.when(z < last)
    def _():
        own_piece(pieces - 1)

    @pl.when(end)
    def _():
        total_copy(True).wait_recv()
        out_t[...] = (g_yin[...] * scale)[:n_taps]

    @pl.when(mid)
    def _():
        out_t[...] = (g_total[...] * scale)[:n_taps]

        @pl.when(z == 1)
        def _():
            total_copy(False).wait_send()

        @pl.when(z == n_z - 2)
        def _():
            total_copy(True).wait_send()


    def all_sent(buf, ss, spare):
        pltpu.make_async_remote_copy(
            src_ref=buf, dst_ref=buf, send_sem=ss, recv_sem=spare,
            device_id=(z * fold + other_y, t), device_id_type=MESH,
        ).wait_send()

    all_sent(got_y.at[:, pl.ds(0, base), :], y_ss.at[0], ly_rs)
    all_sent(got_y.at[pl.ds(0, last), pl.ds(base, swing), :], y_ss.at[1], ly_rs)
    all_sent(got_line.at[pl.ds(0, last), pl.ds(0, base), :], line_ss.at[0], ly_rs)

    def by_place(count):
        all_sent(low_in.at[pl.ds(0, count)], low_ss, ly_rs)
        all_sent(got_line.at[pl.ds(0, count), pl.ds(base, swing), :], line_ss.at[1], ly_rs)

    @pl.when(z < last)
    def _():
        wide_copy.wait_send()
        by_place(last - 1)

    @pl.when(z == last)
    def _():
        by_place(last)


def fused(n_sp, n_tp, proj_value, proj_gate, conv_saved, conv_taps, norm_gain, out_weight, cotangent):
    fold = 2
    n_z = n_sp // fold
    rows, width = cotangent.shape
    ch = conv_saved.shape[1]
    n_taps = conv_taps.shape[0]
    part = width // n_sp
    _, low, wide = split_rows(ch)
    top = ch - low
    sums = -(-2 * (rows // 128) // 8) * 8
    dma = pltpu.SemaphoreType.DMA
    V = pltpu.VMEM
    bf = jnp.bfloat16
    vm = pl.BlockSpec(memory_space=pltpu.VMEM)
    hb = pl.BlockSpec(memory_space=pl.ANY)
    grad_value, grad_gate, grad_weight, grad_taps = pl.pallas_call(
        functools.partial(kernel, n_sp, n_tp, fold),
        out_shape=(V((ch, rows), bf), V((ch, rows), bf), V((ch, part), f32), V((n_taps, ch), f32)),
        in_specs=[hb] * 7,
        out_specs=[vm] * 4,
        scratch_shapes=[
            V((ch, rows), bf), V((n_taps, ch), bf), V((ch,), bf),
            V((ch, rows), bf), V((ch, rows), bf), V((ch, width), bf), V((width, rows), bf), dma((5,)), dma((rows // 128,)), dma((rows // (256 if rows % 256 == 0 else 128),)), pltpu.SemaphoreType.REGULAR,
            V((ch, 128), f32), V((rows, ch), f32), V((rows, ch), f32),
            V((ch, rows), bf), V((ch, rows), f32), V((rows + 32, ch), f32), V((8, rows + 32, ch), f32),
            V((8, rows), f32), V((8, rows), f32),
            V((n_sp, ch, part), f32), V((n_z, top, part), f32), V((n_z + 1, top, part), f32),
            V((n_z + 1, fold, low, part), f32), V((low, part), f32),
            V((sums, 128), f32), V((n_tp - 1, sums, 128), f32),
            V((sums, 128), f32), V((n_tp - 1, sums, 128), f32),
            V((n_taps, 8, ch), f32), *[V((32, ch), f32)] * 8, V((n_taps, 8, ch), f32),
            V((2, 32, ch), f32), V((2, 32, ch), f32), V((8, 128), f32), V((8, 128), f32), V((fold, wide, part), f32), V((wide, part), f32),
            dma, dma, dma, dma, dma((2,)), dma((pieces * n_z,)), dma((2,)), dma((pieces * (n_z + 1),)),
            dma, dma((n_z + 1,)), dma, dma, dma, dma, dma((3,)), dma((3,)), *[dma] * 6, dma((2,)), dma,
        ],
        compiler_params=pltpu.CompilerParams(
            collective_id=0, has_side_effects=True, vmem_limit_bytes=56 * 1024 * 1024
        ),
    )(
        proj_value.T, proj_gate.T, conv_saved.T, conv_taps, norm_gain, out_weight,
        cotangent.T,
    )
    results = (grad_value, grad_gate, grad_weight, grad_taps)
    grad_value, grad_gate, grad_weight, grad_taps = pl.pallas_call(
        finish,
        out_shape=tuple(jax.ShapeDtypeStruct(r.shape, r.dtype) for r in results),
        in_specs=[vm] * 4,
        out_specs=[hb] * 4,
        scratch_shapes=[dma((4,))],
    )(*[pltpu.with_memory_space_constraint(r, pltpu.VMEM) for r in results])
    return grad_value.T, grad_gate.T, grad_weight, grad_taps


def passed_along(block, axis, distance):
    devices = range(lax.axis_size(axis))
    route = [(i - distance, i) for i in devices if i - distance in devices]
    return lax.ppermute(block, axis, route)


def local(proj_value, proj_gate, conv_saved, conv_taps, norm_gain, out_weight, cotangent):
    model_width = cotangent.shape[1]
    tok_rows = cotangent.shape[0]
    tap_count = conv_taps.shape[0]
    overhang = tap_count - 1
    grad_scale = 1.0 / math.sqrt(tok_rows * lax.axis_size("sp"))
    conv_f = conv_saved.astype(jnp.float32)
    totals = lax.psum((jnp.sum(conv_f, axis=1), jnp.sum(conv_f * conv_f, axis=1)), "tp")
    row_mean = totals[0] / model_width
    row_var = totals[1] / model_width - row_mean * row_mean
    inv_std = lax.rsqrt(row_var + norm_eps)
    centered = (conv_f - row_mean[:, None]) * inv_std[:, None]
    gain_f = norm_gain.astype(jnp.float32)
    normed = centered * gain_f
    gate_norm = jax.nn.sigmoid(normed)
    activated = (normed * gate_norm).astype(jnp.bfloat16)
    contract_rows = (((0,), (0,)), ((), ()))
    whole_term = lax.dot_general(
        cotangent, activated, contract_rows, preferred_element_type=jnp.float32
    )
    shard_grad = lax.psum_scatter(whole_term, "sp", scatter_dimension=0, tiled=True)
    grad_out_weight = shard_grad.T * grad_scale
    d_act = lax.dot_general(
        cotangent, out_weight, (((1,), (1,)), ((), ())), preferred_element_type=jnp.float32
    )
    d_hat = d_act * gate_norm * (1.0 + normed * (1.0 - gate_norm)) * gain_f
    moments = lax.psum((jnp.sum(d_hat, axis=1), jnp.sum(d_hat * centered, axis=1)), "tp")
    first = moments[0] / model_width
    second = moments[1] / model_width
    d_conv = inv_std[:, None] * (d_hat - first[:, None] - centered * second[:, None])
    ahead = passed_along(d_conv[:overhang], "sp", -1)
    extended = jnp.concatenate([d_conv, ahead], axis=0)
    gate_proj = jax.nn.sigmoid(proj_gate.astype(jnp.float32))
    gated = proj_value.astype(jnp.float32) * gate_proj
    taps_f = conv_taps.astype(jnp.float32)
    d_glu = jnp.zeros_like(d_conv)
    tap_rows = []
    for offset in range(tap_count):
        shifted = extended[overhang - offset : overhang - offset + tok_rows]
        d_glu = d_glu + taps_f[offset] * shifted
        tap_rows.append(jnp.sum(gated * shifted, axis=0))
    grad_taps = lax.psum(jnp.stack(tap_rows), "sp") * grad_scale
    grad_value = (d_glu * gate_proj).astype(jnp.bfloat16)
    grad_gate = (d_glu * gated * (1.0 - gate_proj)).astype(jnp.bfloat16)
    return (grad_value, grad_gate, grad_out_weight, grad_taps)


def solution(mesh):
    in_specs = (
        P("sp", "tp"),
        P("sp", "tp"),
        P("sp", "tp"),
        P(None, "tp"),
        P("tp"),
        P("tp", None),
        P("sp", None),
    )
    out_specs = (P("sp", "tp"), P("sp", "tp"), P("tp", "sp"), P(None, "tp"))
    n_sp, n_tp = mesh.shape["sp"], mesh.shape["tp"]

    def step(*args):
        rows, width = args[6].shape
        ch, n_taps = args[2].shape[1], args[3].shape[0]
        small = n_sp % 2 == 0 and 6 <= n_sp <= 8 and width % n_sp == 0 and n_tp > 1
        if small and rows % 128 == 0 and rows >= 128 and ch % 8 == 0 and ch >= 64 and 24 < n_taps <= 31:
            return fused(n_sp, n_tp, *args)
        return local(*args)

    return jax.shard_map(step, mesh=mesh, in_specs=in_specs, out_specs=out_specs, check_vma=False)
```

```python
import functools
import math

import jax
import jax.numpy as jnp
from jax import lax
from jax.experimental import pallas as pl
from jax.experimental.pallas import tpu as pltpu
from jax.sharding import PartitionSpec as P

norm_eps = 1e-05
MESH = pl.DeviceIdType.MESH
f32 = jnp.float32
pieces = 4


def line_order(length):
    rows = []
    for place in range(length):
        side = 1 if 2 * place >= length else -1
        rows.append(sorted(range(length), key=lambda d: (-abs(d - place), -side * (d - place))))
    return rows


def split_rows(ch):
    low, wide = ch // 6 // 8 * 8, ch // 21 * 5 // 8 * 8
    units = (ch - wide) // 8
    sizes = [8 * (units // (pieces - 1) + (i < units % (pieces - 1))) for i in range(pieces - 1)]
    return sizes + [wide - low], low, wide


def lookup(table, place):
    value = table[0]
    for i in range(1, len(table)):
        value = jnp.where(place == i, table[i], value)
    return value


def finish(v_in, g_in, w_in, t_in, v_out, g_out, w_out, t_out, ss):
    pairs = [(v_in, v_out), (g_in, g_out), (w_in, w_out), (t_in, t_out)]
    copies = [pltpu.make_async_copy(a, b, ss.at[i]) for i, (a, b) in enumerate(pairs)]
    for c in copies:
        c.start()
    for c in copies:
        c.wait()


def kernel(
    n_sp, n_tp, fold, pv_h, pg_h, conv_h, taps_h, gain_h, weight_h, cot_h,
    out_v, out_g, out_w, out_t,
    conv, taps, gain, pv, pg, weight, cot, in_sems, conv_sems, cot_sems, ready, gain_c, gated_s, d_glu_s, act_t, d_act, ext, shifted, cols, cols2, term, got_y, got_line, low_in, low_y,
    stat, stat_in, mom, mom_in, grad_acc, g_own, g_mid, g_up, g_dn, g_up_out, g_dn_out, g_yin, g_total, taps_b, edge_out, edge_in, edge_sums, edge_sums_in, wide_in, wide_y,
    stat_ss, stat_rs, mom_ss, mom_rs, y_ss, y_rs, line_ss, line_rs,
    low_ss, low_rs, wide_ss, wide_rs, ly_ss, ly_rs, edge_ss, edge_rs,
    gu_ss, gu_rs, gd_ss, gd_rs, gy_ss, gy_rs, gt_ss, gt_rs,
):
    s = lax.axis_index("sp")
    t = lax.axis_index("tp")
    n_z = n_sp // fold
    z = s // fold
    y = s % fold
    other_y = 1 - y
    width, rows = cot.shape
    ch = conv.shape[0]
    part = out_w.shape[1]
    n_taps = taps.shape[0]
    scale = 1.0 / math.sqrt(rows * n_sp)
    blk = 128
    n_blk = rows // blk
    sizes, low, wide = split_rows(ch)
    base, top, swing = ch - wide, ch - low, wide - low
    last = n_z - 1
    end = jnp.logical_or(z == 0, z == n_z - 1)
    mid = jnp.logical_and(z > 0, z < n_z - 1)

    loads = [
        pltpu.make_async_copy(a, b, in_sems.at[i])
        for i, (a, b) in enumerate([
            (weight_h, weight), (pv_h, pv), (pg_h, pg), (gain_h, gain), (taps_h, taps)
        ])
    ]
    conv_loads = [
        pltpu.make_async_copy(
            conv_h.at[:, pl.ds(i * blk, blk)], conv.at[:, pl.ds(i * blk, blk)], conv_sems.at[i]
        )
        for i in range(n_blk)
    ]
    for c in conv_loads:
        c.start()

    barrier = pltpu.get_barrier_semaphore()

    def greet(s_to, t_to):
        pl.semaphore_signal(barrier, inc=1, device_id=(s_to, t_to), device_id_type=MESH)

    for i in range(1, n_tp):
        greet(s, lax.rem(t + i, n_tp))

    @pl.when(y < fold - 1)
    def _():
        greet(s + 1, t)

    @pl.when(z < n_z - 1)
    def _():
        greet(s + fold, t)

        @pl.when(y == fold - 1)
        def _():
            greet(s + 1, t)

    wide_blk = 256 if rows % 256 == 0 else 128
    cot_loads = [
        pltpu.make_async_copy(
            cot_h.at[:, pl.ds(i, wide_blk)], cot.at[:, pl.ds(i, wide_blk)], cot_sems.at[i // wide_blk]
        )
        for i in range(0, rows, wide_blk)
    ]
    loads[3].start()
    loads[0].start()
    for c in cot_loads:
        c.start()

    def put_sums(ref, i, first, second):
        ref[pl.ds(i, 1), :] = jnp.sum(first, axis=0, keepdims=True)
        ref[pl.ds(n_blk + i, 1), :] = jnp.sum(second, axis=0, keepdims=True)

    if stat.shape[0] > 2 * n_blk:
        stat[...] = jnp.zeros_like(stat)
        mom[...] = jnp.zeros_like(mom)

    for i in range(n_blk):
        conv_loads[i].wait()
        c = conv[:, i * blk:(i + 1) * blk].astype(f32)
        put_sums(stat, i, c, c * c)

    first_in_row = jnp.where(y == 0, 1, 0)
    below = jnp.where(z > 0, 1 + first_in_row, 0)
    pl.semaphore_wait(barrier, n_tp - 1 + (1 - first_in_row) + below)

    @pl.when(y > 0)
    def _():
        pl.semaphore_signal(ready, inc=1, device_id=(s - 1, t), device_id_type=MESH)

    @pl.when(z > 0)
    def _():
        pl.semaphore_signal(ready, inc=1, device_id=(s - fold, t), device_id_type=MESH)

    def tp_copies(src, dst, ss, rs):
        return [
            pltpu.make_async_remote_copy(
                src_ref=src, dst_ref=dst.at[i - 1], send_sem=ss, recv_sem=rs,
                device_id=(s, lax.rem(t + i, n_tp)), device_id_type=MESH,
            )
            for i in range(1, n_tp)
        ]

    def tp_wait(dst, ss, rs):
        pltpu.make_async_remote_copy(
            src_ref=dst, dst_ref=dst, send_sem=ss, recv_sem=rs,
            device_id=(s, lax.rem(t + 1, n_tp)), device_id_type=MESH,
        ).wait()

    for c in tp_copies(stat, stat_in, stat_ss, stat_rs):
        c.start()

    reach = 32
    back = jnp.maximum(s - 1, 0)

    def edge_copy(i):
        src, dst = (edge_sums, edge_sums_in) if i == 2 else (edge_out.at[i], edge_in.at[i])
        return pltpu.make_async_remote_copy(
            src_ref=src, dst_ref=dst, send_sem=edge_ss.at[i], recv_sem=edge_rs.at[i],
            device_id=(back, t), device_id_type=MESH,
        )

    def edge_send(i):
        @pl.when(s > 0)
        def _():
            edge_copy(i).start()

    edge_out[0] = conv[:, :blk].astype(f32).T[:reach]
    edge_send(0)
    loads[3].wait()
    gain_c[...] = jnp.broadcast_to(gain[...].astype(f32).reshape(1, ch), (128, ch)).T
    loads[0].wait()
    cot_loads[0].wait()

    d_act[:, :wide_blk] = jnp.dot(weight[...], cot[:, :wide_blk], preferred_element_type=f32)
    edge_out[1] = d_act[:, :blk].T[:reach]
    edge_send(1)

    for i in (1, 2, 4):
        loads[i].start()
    for c in cot_loads[1:]:
        c.wait()
    tp_wait(stat_in, stat_ss, stat_rs)
    total = stat[...]
    for i in range(n_tp - 1):
        total = total + stat_in[i]
    mean = total[:n_blk] / width
    inv = lax.rsqrt(total[n_blk:2 * n_blk] / width - mean * mean + norm_eps)
    for i in range(n_blk):
        cols[0:1, i * blk:(i + 1) * blk] = mean[i:i + 1]
        cols[1:2, i * blk:(i + 1) * blk] = inv[i:i + 1]

    orders = line_order(n_z)
    dest = [lookup([orders[i][k] for i in range(n_z)], z) for k in range(n_z)]

    firsts = [sum(sizes[:h]) for h in range(pieces)]

    def piece(h):
        return pl.ds(firsts[h], sizes[h])

    def y_copy(k, h):
        sem = dest[k] * pieces + h
        return pltpu.make_async_remote_copy(
            src_ref=term.at[dest[k] * fold + other_y, piece(h), :], dst_ref=got_y.at[dest[k], piece(h), :],
            send_sem=y_ss.at[int(h == pieces - 1)], recv_sem=y_rs.at[sem],
            device_id=(z * fold + other_y, t), device_id_type=MESH,
        )

    y_copies = [[y_copy(k, h) for h in range(pieces)] for k in range(n_z)]

    def y_start(k, first=0, past=pieces):
        for h in range(first, past):
            if h < pieces - 1:
                y_copies[k][h].start()
            else:
                @pl.when(dest[k] != last)
                def _():
                    y_copies[k][h].start()

    def make_term(j, at=slice(None)):
        term[j, at, :] = lax.dot_general(
            act_t[at, :], cot[j * part:(j + 1) * part, :], (((1,), (1,)), ((), ())),
            preferred_element_type=f32,
        )

    lead = dest[0] * fold + other_y
    second = dest[0] * fold + y
    leads = sorted({orders[i][0] * fold + o for i in range(n_z) for o in range(fold)})

    def make_one_of(place, at=slice(None)):
        for j in leads:
            @pl.when(place == j)
            def _():
                make_term(j, at)

    def line_copy(d, h, up):
        slot = d + 1 if up else d
        to = z + 1 if up else z - 1
        to = jnp.clip(to, 0, n_z - 1)
        return pltpu.make_async_remote_copy(
            src_ref=term.at[d * fold + y, piece(h), :], dst_ref=got_line.at[slot, piece(h), :],
            send_sem=line_ss.at[int(h == pieces - 1)], recv_sem=line_rs.at[slot * pieces + h],
            device_id=(to * fold + y, t), device_id_type=MESH,
        )

    def add_into(d, h, buf, slot):
        own = d * fold + y
        term[own, piece(h), :] = term[own, piece(h), :] + buf[slot, piece(h), :]

    def line_take(d, h, up):
        line_copy(d, h, up).wait_recv()
        add_into(d, h, got_line, d + 1 if up else d)

    def hop_always(k, h):
        d = dest[k]
        y_copies[k][h].wait_recv()
        add_into(d, h, got_y, d)

        @pl.when(d > z)
        def _():
            @pl.when(z > 0)
            def _():
                line_take(d, h, True)

            line_copy(d, h, True).start()

        @pl.when(d < z)
        def _():
            @pl.when(z < n_z - 1)
            def _():
                line_take(d, h, False)

            line_copy(d, h, False).start()

    def hop(k, h):
        if h < pieces - 1:
            hop_always(k, h)
        else:
            @pl.when(dest[k] != last)
            def _():
                hop_always(k, h)

    def low_copy(d, up):
        slot = d + 1 if up else d
        to = jnp.clip(z + 1 if up else z - 1, 0, n_z - 1)
        return pltpu.make_async_remote_copy(
            src_ref=term.at[pl.ds(d * fold, fold), pl.ds(top, low), :], dst_ref=low_in.at[slot],
            send_sem=low_ss, recv_sem=low_rs.at[slot], device_id=(to * fold + y, t), device_id_type=MESH,
        )

    def low_take(d, up):
        low_copy(d, up).wait_recv()
        at = pl.ds(d * fold, fold)
        term[at, pl.ds(top, low), :] = term[at, pl.ds(top, low), :] + low_in[d + 1 if up else d]

    wide_copy = pltpu.make_async_remote_copy(
        src_ref=term.at[pl.ds(last * fold, fold), pl.ds(base, wide), :], dst_ref=wide_in,
        send_sem=wide_ss, recv_sem=wide_rs,
        device_id=(jnp.clip(z + 1, 0, last) * fold + y, t), device_id_type=MESH,
    )

    def wide_take():
        wide_copy.wait_recv()
        at = slice(last * fold, n_sp)
        term[at, base:, :] = term[at, base:, :] + wide_in[...]

    def low_hop(k):
        d = dest[k]

        @pl.when(d == last)
        def _():
            @pl.when(z > 0)
            def _():
                wide_take()

            wide_copy.start()

        @pl.when(jnp.logical_and(d > z, d < last))
        def _():
            @pl.when(z > 0)
            def _():
                low_take(d, True)

            low_copy(d, True).start()

        @pl.when(d < z)
        def _():
            @pl.when(z < last)
            def _():
                low_take(d, False)

            low_copy(d, False).start()

    def swap_copy(first, count, into):
        return pltpu.make_async_remote_copy(
            src_ref=term.at[z * fold + other_y, pl.ds(first, count), :], dst_ref=into,
            send_sem=ly_ss, recv_sem=ly_rs, device_id=(z * fold + other_y, t), device_id_type=MESH,
        )

    def low_end():
        @pl.when(z < last)
        def _():
            @pl.when(z > 0)
            def _():
                low_take(z, True)

            low_take(z, False)
            swap_copy(top, low, low_y).start()

        @pl.when(z == last)
        def _():
            wide_take()
            swap_copy(base, wide, wide_y).start()

    def activate(at):
        c = conv[at, :].astype(f32)
        gains = jnp.concatenate([gain_c[at, :]] * n_blk, axis=1)
        normed = (c - cols[0:1, :]) * cols[1:2, :] * gains
        act_t[at, :] = (normed * jax.nn.sigmoid(normed)).astype(jnp.bfloat16)

    def lead_piece(h):
        at = slice(firsts[h], firsts[h] + sizes[h])
        activate(at)
        make_one_of(lead, at)
        y_start(0, h, h + 1)


    @pl.when(jnp.logical_or(y == 0, z < n_z - 1))
    def _():
        pl.semaphore_wait(ready, first_in_row + jnp.where(z < n_z - 1, 1, 0))

    @pl.when(mid)
    def _():
        lead_piece(0)

    activate(slice(base, None))
    make_one_of(lead, slice(base, None))
    make_one_of(second, slice(base, None))

    @pl.when(end)
    def _():
        low_hop(0)

    @pl.when(end)
    def _():
        lead_piece(0)

    for h in range(1, pieces - 1):
        lead_piece(h)
    y_start(0, pieces - 1)
    make_one_of(second, slice(0, base))

    for j in range(n_sp):
        if j in leads:
            @pl.when(jnp.logical_and(lead != j, second != j))
            def _():
                make_term(j)
        else:
            make_term(j)

    @pl.when(end)
    def _():
        for k in range(1, n_z - 1):
            low_hop(k)

    @pl.loop(1, rows // wide_blk)
    def _(i):
        at = pl.ds(pl.multiple_of(i * wide_blk, wide_blk), wide_blk)
        d_act[:, at] = jnp.dot(weight[...], cot[:, at], preferred_element_type=f32)

    @pl.loop(0, n_blk)
    def _(i):
        at = pl.ds(pl.multiple_of(i * blk, blk), blk)
        c = conv[:, at].astype(f32)
        centered = (c - cols[0:1, at]) * cols[1:2, at]
        normed = centered * gain_c[...]
        gate = jax.nn.sigmoid(normed)
        d_hat = d_act[:, at] * gate * (1.0 + normed * (1.0 - gate)) * gain_c[...]
        d_act[:, at] = d_hat
        put_sums(mom, i, d_hat, d_hat * centered)

    for c in tp_copies(mom, mom_in, mom_ss, mom_rs):
        c.start()
    loads[4].wait()
    for k in range(n_taps):
        taps_b[k] = jnp.broadcast_to(taps[k:k + 1, :].astype(f32), (8, ch))
    grad_acc[...] = jnp.zeros_like(grad_acc)
    loads[1].wait()
    loads[2].wait()

    @pl.loop(0, n_blk)
    def _(i):
        at = pl.ds(pl.multiple_of(i * blk, blk), blk)
        gated_s[at, :] = (pv[:, at].astype(f32) * jax.nn.sigmoid(pg[:, at].astype(f32))).T

    tp_wait(mom_in, mom_ss, mom_rs)
    total = mom[...]
    for i in range(n_tp - 1):
        total = total + mom_in[i]
    total = total / width
    for i in range(n_blk):
        cols2[0:1, i * blk:(i + 1) * blk] = total[i:i + 1]
        cols2[1:2, i * blk:(i + 1) * blk] = total[n_blk + i:n_blk + i + 1]

    edge_sums[...] = jnp.zeros_like(edge_sums)
    edge_sums[0:2, :] = cols[0:2, :blk]
    edge_sums[2:4, :] = cols2[0:2, :blk]
    edge_send(2)
    y_start(1)

    @pl.loop(0, n_blk)
    def _(i):
        at = pl.ds(pl.multiple_of(i * blk, blk), blk)
        c = conv[:, at].astype(f32)
        inv_std = cols[1:2, at]
        centered = (c - cols[0:1, at]) * inv_std
        ext[at, :] = (inv_std * (d_act[:, at] - cols2[0:1, at] - centered * cols2[1:2, at])).T

    def shift_block(i):
        start = pl.multiple_of(i * reach, reach)
        win = ext[pl.ds(start, reach + 8), :]
        for o in range(8):
            shifted[o, pl.ds(start, reach), :] = win[o:o + reach]

    lanes = [(lo, min(128, ch - lo)) for lo in range(0, ch, 128)]

    def conv_blocks(first, last):
        for lo, wide in lanes:
            ln = slice(lo, lo + wide)

            def body(i, accs):
                start = pl.multiple_of(i * reach, reach)
                at = pl.ds(start, reach)
                gated = gated_s[at, ln]
                d_glu = jnp.zeros((reach, wide), f32)
                out = []
                for o in range(n_taps):
                    x = shifted[o % 8, pl.ds(pl.multiple_of(start + 8 * (o // 8), 8), reach), ln]
                    tap = taps_b[n_taps - 1 - o, :, ln]
                    d_glu = d_glu + jnp.concatenate([tap] * (reach // 8), axis=0) * x
                    prod = gated * x
                    acc = accs[o]
                    for q in range(reach // 8):
                        acc = acc + prod[8 * q:8 * q + 8]
                    out.append(acc)
                d_glu_s[at, ln] = d_glu
                return tuple(out)

            accs = tuple(grad_acc[n_taps - 1 - o, :, ln] for o in range(n_taps))
            accs = lax.fori_loop(first, last, body, accs)
            for o in range(n_taps):
                grad_acc[n_taps - 1 - o, :, ln] = accs[o]

    n_row = rows // reach

    @pl.loop(0, n_row - 1)
    def _(i):
        shift_block(i)

    half = (n_row - 2) // 2
    conv_blocks(0, half)

    @pl.when(end)
    def _():
        hop(0, 0)
        hop(0, 1)

    @pl.when(mid)
    def _():
        low_hop(0)

    conv_blocks(half, n_row - 2)

    @pl.when(s < n_sp - 1)
    def _():
        for i in range(3):
            edge_copy(i).wait_recv()
        per_token = edge_sums_in[...].T[:reach]
        mean_e, inv_e, first_e, second_e = [per_token[:, i:i + 1] for i in range(4)]
        gain_e = gain[...].astype(f32).reshape(1, ch)
        centered = (edge_in[0] - mean_e) * inv_e
        normed = centered * gain_e
        gate = jax.nn.sigmoid(normed)
        d_hat = edge_in[1] * gate * (1.0 + normed * (1.0 - gate)) * gain_e
        ext[pl.ds(rows, reach), :] = inv_e * (d_hat - first_e - centered * second_e)

    @pl.when(s == n_sp - 1)
    def _():
        ext[pl.ds(rows, reach), :] = jnp.zeros((reach, ch), f32)

    shift_block(n_row - 1)
    win = ext[pl.ds(rows, reach), :]
    for o in range(8):
        shifted[o, pl.ds(rows, reach - 8), :] = win[o:o + reach - 8]
    conv_blocks(n_row - 2, n_row)

    for k in range(n_taps):
        g_own[k:k + 1, :] = jnp.sum(grad_acc[k], axis=0, keepdims=True)
    for k in range(n_taps, g_own.shape[0]):
        g_own[k:k + 1, :] = jnp.zeros((1, ch), f32)

    def taps_copy(src, up):
        dst, ss, rs = (g_up, gu_ss, gu_rs) if up else (g_dn, gd_ss, gd_rs)
        to = jnp.clip(z + 1 if up else z - 1, 0, n_z - 1)
        return pltpu.make_async_remote_copy(
            src_ref=src, dst_ref=dst, send_sem=ss, recv_sem=rs,
            device_id=(to * fold + y, t), device_id_type=MESH,
        )

    def taps_pass(up):
        src = g_up if up else g_dn
        out = g_up_out if up else g_dn_out
        taps_copy(g_own, up).wait_recv()

        @pl.when(z < n_z - 2 if up else z > 1)
        def _():
            out[...] = g_own[...] + src[...]
            taps_copy(out, up).start()

    @pl.when(z == 0)
    def _():
        taps_copy(g_own, True).start()

    @pl.when(z == n_z - 1)
    def _():
        taps_copy(g_own, False).start()

    y_start(2, 0, pieces if n_z > 3 else 2)

    @pl.loop(0, n_blk)
    def _(i):
        at = pl.ds(pl.multiple_of(i * blk, blk), blk)
        gate = jax.nn.sigmoid(pg[:, at].astype(f32))
        d_glu = d_glu_s[at, :].T
        out_v[:, at] = (d_glu * gate).astype(jnp.bfloat16)
        out_g[:, at] = (d_glu * (pv[:, at].astype(f32) * gate) * (1.0 - gate)).astype(jnp.bfloat16)

    @pl.when(end)
    def _():
        hop(0, 2)
        hop(0, 3)
        for k in range(1, n_z - 2):
            for h in range(pieces):
                hop(k, h)

    @pl.when(mid)
    def _():
        for k in range(n_z - 2, 0, -1):
            low_hop(k)
        hop(0, 0)
        hop(0, 1)

        @pl.when(2 * z < n_z)
        def _():
            taps_pass(True)

        @pl.when(2 * z >= n_z)
        def _():
            taps_pass(False)

        hop(0, 2)
        hop(0, 3)

    low_end()
    gy = pltpu.make_async_remote_copy(
        src_ref=g_mid, dst_ref=g_yin, send_sem=gy_ss, recv_sem=gy_rs,
        device_id=(z * fold + other_y, t), device_id_type=MESH,
    )

    def total_copy(up):
        to = jnp.clip(z + 1 if up else z - 1, 0, n_z - 1)
        return pltpu.make_async_remote_copy(
            src_ref=g_total, dst_ref=g_yin, send_sem=gt_ss.at[int(up)], recv_sem=gt_rs,
            device_id=(to * fold + y, t), device_id_type=MESH,
        )

    y_start(n_z - 1, 0, 1)

    @pl.when(end)
    def _():
        y_start(n_z - 1, 1, pieces)

    @pl.when(end)
    def _():
        for h in range(pieces):
            hop(n_z - 2, h)

    @pl.when(mid)
    def _():
        @pl.when(2 * z < n_z)
        def _():
            taps_pass(False)

        @pl.when(2 * z >= n_z)
        def _():
            taps_pass(True)

        g_mid[...] = g_own[...] + g_up[...] + g_dn[...]
        gy.start()
        y_start(n_z - 1, 1, pieces)
        later = [(k, h) for k in range(1, n_z - 1) for h in range(pieces)]
        for k, h in sorted(later, key=lambda p: (p[1] + 2 * p[0], p[0])):
            hop(k, h)


    @pl.when(z < n_z - 2)
    def _():
        taps_copy(g_own, True).wait_send()

    @pl.when(z > 1)
    def _():
        taps_copy(g_own, False).wait_send()

    @pl.when(s > 0)
    def _():
        for i in range(3):
            edge_copy(i).wait_send()

    own = z * fold + y

    @pl.when(z < last)
    def _():
        swap_copy(top, low, low_y).wait()
        out_w[top:, :] = (term[own, top:, :] + low_y[...]) * scale

    @pl.when(z == last)
    def _():
        swap_copy(base, wide, wide_y).wait()
        out_w[base:, :] = (term[own, base:, :] + wide_y[...]) * scale

    def own_piece(h):
        y_copies[last][h].wait_recv()
        add_into(z, h, got_y, z)

        @pl.when(z > 0)
        def _():
            line_take(z, h, True)

        @pl.when(z < last)
        def _():
            line_take(z, h, False)

        out_w[piece(h), :] = term[own, piece(h), :] * scale

    @pl.when(mid)
    def _():
        gy.wait()
        g_total[...] = g_mid[...] + g_yin[...]

        @pl.when(z == 1)
        def _():
            total_copy(False).start()

        @pl.when(z == n_z - 2)
        def _():
            total_copy(True).start()

    for h in range(pieces - 1):
        own_piece(h)

    @pl.when(z < last)
    def _():
        own_piece(pieces - 1)

    @pl.when(end)
    def _():
        total_copy(True).wait_recv()
        out_t[...] = (g_yin[...] * scale)[:n_taps]

    @pl.when(mid)
    def _():
        out_t[...] = (g_total[...] * scale)[:n_taps]

        @pl.when(z == 1)
        def _():
            total_copy(False).wait_send()

        @pl.when(z == n_z - 2)
        def _():
            total_copy(True).wait_send()


    def all_sent(buf, ss, spare):
        pltpu.make_async_remote_copy(
            src_ref=buf, dst_ref=buf, send_sem=ss, recv_sem=spare,
            device_id=(z * fold + other_y, t), device_id_type=MESH,
        ).wait_send()

    all_sent(got_y.at[:, pl.ds(0, base), :], y_ss.at[0], ly_rs)
    all_sent(got_y.at[pl.ds(0, last), pl.ds(base, swing), :], y_ss.at[1], ly_rs)
    all_sent(got_line.at[pl.ds(0, last), pl.ds(0, base), :], line_ss.at[0], ly_rs)

    def by_place(count):
        all_sent(low_in.at[pl.ds(0, count)], low_ss, ly_rs)
        all_sent(got_line.at[pl.ds(0, count), pl.ds(base, swing), :], line_ss.at[1], ly_rs)

    @pl.when(z < last)
    def _():
        wide_copy.wait_send()
        by_place(last - 1)

    @pl.when(z == last)
    def _():
        by_place(last)


def fused(n_sp, n_tp, proj_value, proj_gate, conv_saved, conv_taps, norm_gain, out_weight, cotangent):
    fold = 2
    n_z = n_sp // fold
    rows, width = cotangent.shape
    ch = conv_saved.shape[1]
    n_taps = conv_taps.shape[0]
    part = width // n_sp
    _, low, wide = split_rows(ch)
    top = ch - low
    sums = -(-2 * (rows // 128) // 8) * 8
    dma = pltpu.SemaphoreType.DMA
    V = pltpu.VMEM
    bf = jnp.bfloat16
    vm = pl.BlockSpec(memory_space=pltpu.VMEM)
    hb = pl.BlockSpec(memory_space=pl.ANY)
    grad_value, grad_gate, grad_weight, grad_taps = pl.pallas_call(
        functools.partial(kernel, n_sp, n_tp, fold),
        out_shape=(V((ch, rows), bf), V((ch, rows), bf), V((ch, part), f32), V((n_taps, ch), f32)),
        in_specs=[hb] * 7,
        out_specs=[vm] * 4,
        scratch_shapes=[
            V((ch, rows), bf), V((n_taps, ch), bf), V((ch,), bf),
            V((ch, rows), bf), V((ch, rows), bf), V((ch, width), bf), V((width, rows), bf), dma((5,)), dma((rows // 128,)), dma((rows // (256 if rows % 256 == 0 else 128),)), pltpu.SemaphoreType.REGULAR,
            V((ch, 128), f32), V((rows, ch), f32), V((rows, ch), f32),
            V((ch, rows), bf), V((ch, rows), f32), V((rows + 32, ch), f32), V((8, rows + 32, ch), f32),
            V((8, rows), f32), V((8, rows), f32),
            V((n_sp, ch, part), f32), V((n_z, top, part), f32), V((n_z + 1, top, part), f32),
            V((n_z + 1, fold, low, part), f32), V((low, part), f32),
            V((sums, 128), f32), V((n_tp - 1, sums, 128), f32),
            V((sums, 128), f32), V((n_tp - 1, sums, 128), f32),
            V((n_taps, 8, ch), f32), *[V((32, ch), f32)] * 8, V((n_taps, 8, ch), f32),
            V((2, 32, ch), f32), V((2, 32, ch), f32), V((8, 128), f32), V((8, 128), f32), V((fold, wide, part), f32), V((wide, part), f32),
            dma, dma, dma, dma, dma((2,)), dma((pieces * n_z,)), dma((2,)), dma((pieces * (n_z + 1),)),
            dma, dma((n_z + 1,)), dma, dma, dma, dma, dma((3,)), dma((3,)), *[dma] * 6, dma((2,)), dma,
        ],
        compiler_params=pltpu.CompilerParams(
            collective_id=0, has_side_effects=True, vmem_limit_bytes=56 * 1024 * 1024
        ),
    )(
        proj_value.T, proj_gate.T, conv_saved.T, conv_taps, norm_gain, out_weight,
        cotangent.T,
    )
    results = (grad_value, grad_gate, grad_weight, grad_taps)
    grad_value, grad_gate, grad_weight, grad_taps = pl.pallas_call(
        finish,
        out_shape=tuple(jax.ShapeDtypeStruct(r.shape, r.dtype) for r in results),
        in_specs=[vm] * 4,
        out_specs=[hb] * 4,
        scratch_shapes=[dma((4,))],
    )(*[pltpu.with_memory_space_constraint(r, pltpu.VMEM) for r in results])
    return grad_value.T, grad_gate.T, grad_weight, grad_taps


def passed_along(block, axis, distance):
    devices = range(lax.axis_size(axis))
    route = [(i - distance, i) for i in devices if i - distance in devices]
    return lax.ppermute(block, axis, route)


def local(proj_value, proj_gate, conv_saved, conv_taps, norm_gain, out_weight, cotangent):
    model_width = cotangent.shape[1]
    tok_rows = cotangent.shape[0]
    tap_count = conv_taps.shape[0]
    overhang = tap_count - 1
    grad_scale = 1.0 / math.sqrt(tok_rows * lax.axis_size("sp"))
    conv_f = conv_saved.astype(jnp.float32)
    totals = lax.psum((jnp.sum(conv_f, axis=1), jnp.sum(conv_f * conv_f, axis=1)), "tp")
    row_mean = totals[0] / model_width
    row_var = totals[1] / model_width - row_mean * row_mean
    inv_std = lax.rsqrt(row_var + norm_eps)
    centered = (conv_f - row_mean[:, None]) * inv_std[:, None]
    gain_f = norm_gain.astype(jnp.float32)
    normed = centered * gain_f
    gate_norm = jax.nn.sigmoid(normed)
    activated = (normed * gate_norm).astype(jnp.bfloat16)
    contract_rows = (((0,), (0,)), ((), ()))
    whole_term = lax.dot_general(
        cotangent, activated, contract_rows, preferred_element_type=jnp.float32
    )
    shard_grad = lax.psum_scatter(whole_term, "sp", scatter_dimension=0, tiled=True)
    grad_out_weight = shard_grad.T * grad_scale
    d_act = lax.dot_general(
        cotangent, out_weight, (((1,), (1,)), ((), ())), preferred_element_type=jnp.float32
    )
    d_hat = d_act * gate_norm * (1.0 + normed * (1.0 - gate_norm)) * gain_f
    moments = lax.psum((jnp.sum(d_hat, axis=1), jnp.sum(d_hat * centered, axis=1)), "tp")
    first = moments[0] / model_width
    second = moments[1] / model_width
    d_conv = inv_std[:, None] * (d_hat - first[:, None] - centered * second[:, None])
    ahead = passed_along(d_conv[:overhang], "sp", -1)
    extended = jnp.concatenate([d_conv, ahead], axis=0)
    gate_proj = jax.nn.sigmoid(proj_gate.astype(jnp.float32))
    gated = proj_value.astype(jnp.float32) * gate_proj
    taps_f = conv_taps.astype(jnp.float32)
    d_glu = jnp.zeros_like(d_conv)
    tap_rows = []
    for offset in range(tap_count):
        shifted = extended[overhang - offset : overhang - offset + tok_rows]
        d_glu = d_glu + taps_f[offset] * shifted
        tap_rows.append(jnp.sum(gated * shifted, axis=0))
    grad_taps = lax.psum(jnp.stack(tap_rows), "sp") * grad_scale
    grad_value = (d_glu * gate_proj).astype(jnp.bfloat16)
    grad_gate = (d_glu * gated * (1.0 - gate_proj)).astype(jnp.bfloat16)
    return (grad_value, grad_gate, grad_out_weight, grad_taps)


def solution(mesh):
    in_specs = (
        P("sp", "tp"),
        P("sp", "tp"),
        P("sp", "tp"),
        P(None, "tp"),
        P("tp"),
        P("tp", None),
        P("sp", None),
    )
    out_specs = (P("sp", "tp"), P("sp", "tp"), P("tp", "sp"), P(None, "tp"))
    n_sp, n_tp = mesh.shape["sp"], mesh.shape["tp"]

    def step(*args):
        rows, width = args[6].shape
        ch, n_taps = args[2].shape[1], args[3].shape[0]
        small = n_sp % 2 == 0 and 6 <= n_sp <= 8 and width % n_sp == 0 and n_tp > 1
        if small and rows % 128 == 0 and rows >= 128 and ch % 8 == 0 and ch >= 64 and 24 < n_taps <= 31:
            return fused(n_sp, n_tp, *args)
        return local(*args)

    return jax.shard_map(step, mesh=mesh, in_specs=in_specs, out_specs=out_specs, check_vma=False)
```
